512 devices in a mesh: sp: 32 (over z, core), tp: 16 (over y, x).
Axes of the slice: x: 4, y: 4, z: 16, core: 2. Of those that a mesh axis runs over, the one named last changes fastest.
Arguments:
- receptance: bfloat16 [8192, 4096], P('sp', 'tp'), may hold values from -6 to 6
- key_vectors: bfloat16 [8192, 4096], P('sp', 'tp'), may hold values from -13 to 13
- value_vectors: bfloat16 [8192, 4096], P('sp', 'tp'), may hold values from -6 to 6
- decay_logits: bfloat16 [8192, 4096], P('sp', 'tp'), may hold values from -20 to 2
- rate_logits: bfloat16 [8192, 4096], P('sp', 'tp'), may hold values from -8 to 4
- gate_logits: bfloat16 [8192, 4096], P('sp', 'tp'), may hold values from -6 to 6
- group_gain: float32 [4096], P('tp'), may hold values from 0.1 to 1.9
- residual: bfloat16 [8192, 4096], P('sp', 'tp'), may hold values from -24 to 24
- mixer_out: bfloat16 [4096, 4096], P(None, 'tp'), may hold values from -0.09375 to 0.09375
- norm_gain: float32 [4096], P('tp'), may hold values from 0.1 to 1.9
- expert_ids: int32 [8192, 2], P('sp'), may hold values from 0 to 31, as said below
- route_weight: float32 [8192, 2], P('sp'), may hold values from 0.25 to 1
- expert_gate: bfloat16 [32, 4096, 1024], P('sp', 'tp'), may hold values from -0.09375 to 0.09375
- expert_up: bfloat16 [32, 4096, 1024], P('sp', 'tp'), may hold values from -0.09375 to 0.09375
- expert_down: bfloat16 [32, 1024, 4096], P('sp', None, 'tp'), may hold values from -0.1875 to 0.1875
Outputs:
- updated: bfloat16 [8192, 4096], P('sp', 'tp')
The draws below stay inside these ranges and needn't reach their ends.
Inputs may be any that keep to these rules, and one draw needn't show every extreme that they name: `expert_ids`: the experts of a row are different and lie in one group of 8 consecutive experts. In the rows of one index of sp (aligned blocks of 256 rows) no expert is named by more than 32 rows, and in every such block some expert is named by exactly 32 rows.
All inputs are finite; a program needn't handle non-finite values.
Results may differ from the reference program's by a relative error of at most 0.013.
Values may be sent and summed in bfloat16 or wider, within the bound.
A program may use at most 64 MiB of HBM per device.

```python
import math
import jax
import jax.numpy as jnp
from jax import lax

D = 4096
WIDTH = 4096
HEAD = 64
HEADS = 64
FF = 1024
GROUPS = 4
TOP = 2
TOK_SP = 256
EXPERTS = 32
GROUP_EXPERTS = 8
CAP = 32
SLOTS = 1024
TOKENS = 8192
CUTS = 16
DBLK = 256
N_SP = 32


def fast_heads(key, count):
    order = jax.random.permutation(jax.random.fold_in(key, 7101), HEADS)
    return order < count


def draw_decay_logits(key, part):
    flags = fast_heads(key, HEADS // 2)
    noise = 0.6 * jnp.clip(jax.random.normal(jax.random.fold_in(key, 2), (TOKENS, WIDTH), jnp.float32), -3.0, 3.0)
    per_head = jnp.where(flags, math.log(1.0 / 16.0), math.log(0.8 / TOKENS))
    base = jnp.repeat(per_head, HEAD)
    channel = 0.3 * jnp.clip(jax.random.normal(jax.random.fold_in(key, 3), (WIDTH,), jnp.float32), -3.0, 3.0)
    halves = TOKENS // (TOK_SP // 2)
    drift = jax.random.uniform(jax.random.fold_in(key, 4), (halves, 1), jnp.float32, -1.1, 1.1)
    drift = jnp.repeat(drift, TOK_SP // 2, axis=0)
    log_rate = jnp.minimum(base[None, :] + channel[None, :] + drift + noise, -0.7)
    shifted = log_rate + 0.5
    return (shifted - jnp.log1p(-jnp.exp(shifted))).astype(jnp.bfloat16)


def draw_rate_logits(key, part):
    flags = fast_heads(key, HEADS // 2)
    spread = 0.7 * jnp.clip(jax.random.normal(jax.random.fold_in(key, 5), (TOKENS, WIDTH), jnp.float32), -2.4, 2.4)
    mixed_channels = jax.random.bernoulli(jax.random.fold_in(key, 6), 0.5, (WIDTH,))
    strong = jnp.logical_or(jnp.repeat(flags, HEAD), mixed_channels)
    centre = jnp.where(strong, 2.3, -6.0)
    width_scale = jnp.where(strong, 1.0, 0.5)
    return (centre[None, :] + width_scale[None, :] * spread).astype(jnp.bfloat16)


def draw_key_vectors(key, part):
    direction = jnp.clip(jax.random.normal(jax.random.fold_in(key, 21), (HEADS, HEAD), jnp.float32), -3.0, 3.0)
    along = 1.0 + 0.4 * jnp.clip(jax.random.normal(jax.random.fold_in(key, 22), (TOKENS, HEADS), jnp.float32), -2.0, 2.0)
    rough = jnp.clip(jax.random.normal(jax.random.fold_in(key, 23), (TOKENS, HEADS, HEAD), jnp.float32), -4.0, 4.0)
    keys = 1.5 * along[:, :, None] * direction[None, :, :] + rough
    return keys.reshape(TOKENS, WIDTH).astype(jnp.bfloat16)


def draw_residual(key, part):
    column_blocks = max(D // 128, 1)
    scales = jnp.exp(jax.random.uniform(jax.random.fold_in(key, 11), (column_blocks,), jnp.float32, math.log(0.4), math.log(2.5)))
    scales = jnp.repeat(scales, D // column_blocks)
    base = jnp.clip(jax.random.normal(jax.random.fold_in(key, 12), (TOKENS, D), jnp.float32), -5.0, 5.0)
    return (base * scales[None, :]).astype(jnp.bfloat16)


def draw_expert_ids(key, part):
    anchor = jax.random.fold_in(key, 9001)
    full_group = jax.random.randint(jax.random.fold_in(anchor, 1), (), 0, GROUPS)
    full_lead = jax.random.randint(jax.random.fold_in(anchor, 2), (), 0, GROUP_EXPERTS)
    block_keys = jax.random.split(jax.random.fold_in(anchor, 3), TOKENS // TOK_SP)
    spots = jnp.arange(GROUPS, dtype=jnp.int32)
    others_width = max(GROUP_EXPERTS - 1, 1)

    def one_block(block_key):
        keys_here = jax.random.split(block_key, 5)
        order = jax.random.permutation(keys_here[0], TOK_SP).astype(jnp.int32)
        held = jax.random.randint(keys_here[1], (), CAP, TOK_SP // 2 + 1)
        shift = jax.random.randint(keys_here[2], (), 0, GROUPS - 1)
        leads = jax.random.randint(keys_here[3], (GROUPS,), 0, GROUP_EXPERTS)
        leads = jnp.where(spots == full_group, full_lead, leads)
        shuffles = jax.vmap(lambda subkey: jax.random.permutation(subkey, others_width))(jax.random.split(keys_here[4], GROUPS)).astype(jnp.int32)
        in_full = order < held
        others = order - held
        group = jnp.where(in_full, full_group, (full_group + 1 + (others + shift) % (GROUPS - 1)) % GROUPS)
        rank = jnp.where(in_full, order, others // (GROUPS - 1))
        lead = leads[group]
        shuffle_rows = shuffles[group]

        def other_expert(position):
            pick = jnp.take_along_axis(shuffle_rows, (position % others_width)[:, None], axis=1)[:, 0]
            return (lead + 1 + pick) % GROUP_EXPERTS
        early = rank < CAP
        late_pos = CAP + 2 * (rank - CAP)
        first_pick = jnp.where(early, lead, other_expert(late_pos))
        second_pick = jnp.where(early, other_expert(rank), other_expert(late_pos + 1))
        return jnp.stack([group * GROUP_EXPERTS + first_pick, group * GROUP_EXPERTS + second_pick], axis=1)
    chosen = jax.vmap(one_block)(block_keys)
    return chosen.reshape(TOKENS, TOP).astype(jnp.int32)


def block_levels(own_key, extent, pieces, least, top_value):
    def one(dim, parts):
        steps = jax.random.uniform(jax.random.fold_in(jax.random.fold_in(own_key, 6), dim), (parts,), jnp.float32, least / len(pieces), top_value / len(pieces))
        return jnp.repeat(jnp.exp(steps), extent[dim] // parts).reshape((-1,) + (1,) * (len(extent) - dim - 1))

    loudness = one(*pieces[0])
    for cut in pieces[1:]:
        loudness = loudness * one(*cut)
    return loudness


def normal_values(key, dims, width, bound, cuts=(), kind=jnp.bfloat16):
    values = jax.random.normal(key, dims, jnp.float32) * width
    if len(cuts) > 0:
        values = block_levels(key, dims, cuts, -0.22, 0.18) * values
    return jnp.clip(values, min=-bound, max=bound).astype(kind)


def setup_inputs(seed: int = 0) -> dict:
    key_list = jax.random.split(jax.random.key(seed), 16)
    return {
        "receptance": normal_values(key_list[0], (TOKENS, WIDTH), 1.0, 6.0, ((0, 32), (1, 16))),
        "key_vectors": draw_key_vectors(jax.random.fold_in(key_list[15], 71), 0),
        "value_vectors": normal_values(key_list[2], (TOKENS, WIDTH), 1.0, 6.0, ((0, 32), (1, 16))),
        "decay_logits": draw_decay_logits(jax.random.fold_in(key_list[15], 71), 0),
        "rate_logits": draw_rate_logits(jax.random.fold_in(key_list[15], 71), 0),
        "gate_logits": normal_values(key_list[5], (TOKENS, WIDTH), 1.5, 6.0, ((0, 32), (1, 16))),
        "group_gain": jnp.clip(1.0 + 0.18 * jax.random.normal(key_list[6], (WIDTH,), jnp.float32), 0.1, 1.9),
        "residual": draw_residual(jax.random.fold_in(key_list[15], 71), 0),
        "mixer_out": normal_values(key_list[8], (WIDTH, D), WIDTH ** -0.5, 0.09375, ((1, 16),)),
        "norm_gain": jnp.clip(1.0 + 0.18 * jax.random.normal(key_list[9], (D,), jnp.float32), 0.1, 1.9),
        "expert_ids": draw_expert_ids(jax.random.fold_in(key_list[15], 71), 0),
        "route_weight": jnp.clip(0.25 + 0.75 * jax.random.uniform(key_list[11], (TOKENS, TOP), jnp.float32) ** block_levels(key_list[11], (TOKENS, TOP), ((0, 32),), -0.2, 0.2), 0.25, 1.0),
        "expert_gate": normal_values(key_list[12], (EXPERTS, D, FF), D ** -0.5, 0.09375, ((0, 32), (1, 16))),
        "expert_up": normal_values(key_list[13], (EXPERTS, D, FF), D ** -0.5, 0.09375, ((0, 32), (1, 16))),
        "expert_down": normal_values(key_list[14], (EXPERTS, FF, D), FF ** -0.5, 0.1875, ((0, 32), (2, 16))),
    }


EPS_GROUP = 0.00064
EPS_NORM = 1e-06
HIGHEST = lax.Precision.HIGHEST

def by_heads(array):
    return array.astype(jnp.float32).reshape(array.shape[0], WIDTH // HEAD, HEAD)

def time_mix(receptance, key_vectors, value_vectors, decay_logits, rate_logits, gate_logits, group_gain):
    recept = by_heads(receptance)
    keyvec = by_heads(key_vectors)
    valvec = by_heads(value_vectors)
    decay = jnp.exp(-jnp.exp(-jax.nn.softplus(-by_heads(decay_logits)) - 0.5))
    unit_key = keyvec / jnp.sqrt(1.0 + lax.optimization_barrier(jnp.sum(keyvec * keyvec, axis=-1, keepdims=True)))
    correction = unit_key * jax.nn.sigmoid(by_heads(rate_logits))

    def advance(carried, inputs):
        recept_now, decay_now, key_now, value_now, unit_now, corr_now = inputs
        pulled = jnp.einsum('hij,hj->hi', carried, unit_now, precision=HIGHEST)
        carried = carried * decay_now[:, None, :] - pulled[:, :, None] * corr_now[:, None, :] + value_now[:, :, None] * key_now[:, None, :]
        return (carried, jnp.einsum('hij,hj->hi', carried, recept_now, precision=HIGHEST))
    initial = jnp.zeros((WIDTH // HEAD, HEAD, HEAD), jnp.float32)
    final_state, state_read = lax.scan(advance, initial, (recept, decay, keyvec, valvec, unit_key, correction))
    centred = state_read - lax.optimization_barrier(jnp.mean(state_read, axis=-1, keepdims=True))
    scaled = centred * lax.rsqrt(lax.optimization_barrier(jnp.mean(centred * centred, axis=-1, keepdims=True)) + EPS_GROUP)
    gated_out = scaled.reshape(TOKENS, WIDTH) * group_gain.astype(jnp.float32)[None, :] * jax.nn.sigmoid(gate_logits.astype(jnp.float32))
    return gated_out.astype(jnp.bfloat16)

def block_ranks(expert_ids):
    grouped = expert_ids.reshape(N_SP, TOK_SP * TOP)
    onehot = (grouped[:, :, None] == jnp.arange(EXPERTS, dtype=jnp.int32)[None, None, :]).astype(jnp.int32)
    earlier = jnp.cumsum(onehot, axis=1) - onehot
    return lax.optimization_barrier(jnp.sum(earlier * onehot, axis=2)).reshape(TOKENS, TOP).astype(jnp.int32)

def cut_product(chosen, matrix):
    rows_cut = chosen.astype(jnp.float32).reshape(chosen.shape[0], CUTS, DBLK)
    matrix_cut = matrix.astype(jnp.float32).reshape(CUTS, DBLK, matrix.shape[1])
    partials = jnp.einsum('scd,cdf->csf', rows_cut, matrix_cut)
    rounded = lax.optimization_barrier(partials.astype(jnp.bfloat16))
    return lax.optimization_barrier(jnp.sum(rounded.astype(jnp.float32), axis=0))

def reference(receptance, key_vectors, value_vectors, decay_logits, rate_logits, gate_logits, group_gain, residual, mixer_out, norm_gain, expert_ids, route_weight, expert_gate, expert_up, expert_down):
    mixed_rows = time_mix(receptance, key_vectors, value_vectors, decay_logits, rate_logits, gate_logits, group_gain)
    midway = (residual.astype(jnp.float32) + jnp.dot(mixed_rows, mixer_out, preferred_element_type=jnp.float32)).astype(jnp.bfloat16)
    midway_f = midway.astype(jnp.float32)
    inv_rms = lax.rsqrt(lax.optimization_barrier(jnp.mean(midway_f * midway_f, axis=1, keepdims=True)) + EPS_NORM)
    normed = (midway_f * norm_gain.astype(jnp.float32)[None, :] * inv_rms).astype(jnp.bfloat16)
    ranks = block_ranks(expert_ids)
    token_ids = jnp.arange(TOKENS, dtype=jnp.int32)
    within = ((token_ids // TOK_SP)[:, None] * CAP + ranks).astype(jnp.int32)
    owners = jnp.broadcast_to(token_ids[:, None], expert_ids.shape).astype(jnp.int32)
    slot_table = jnp.full((EXPERTS, SLOTS), TOKENS, jnp.int32).at[expert_ids, within].set(owners)
    slot_weight = jnp.zeros((EXPERTS, SLOTS), jnp.float32).at[expert_ids, within].set(route_weight.astype(jnp.float32))
    padded = jnp.concatenate([normed, jnp.zeros((1, D), jnp.bfloat16)], axis=0)

    def one_expert(running, inputs):
        table_row, weight_row, gate_mat, up_mat, down_mat = inputs
        chosen = padded[table_row]
        hidden = (jax.nn.silu(cut_product(chosen, gate_mat)) * cut_product(chosen, up_mat)).astype(jnp.bfloat16)
        result = jnp.dot(hidden, down_mat, preferred_element_type=jnp.float32).astype(jnp.bfloat16)
        running = running.at[table_row].add(result.astype(jnp.float32) * weight_row[:, None])
        return (running, None)
    routed, unused = lax.scan(one_expert, jnp.zeros((TOKENS + 1, D), jnp.float32), (slot_table, slot_weight, expert_gate, expert_up, expert_down))
    return (midway_f + routed[:TOKENS]).astype(jnp.bfloat16)
```

```python
import jax
import jax.numpy as jnp
from jax import lax
from jax.experimental import pallas as pl
from jax.experimental.pallas import tpu as pltpu
from jax.sharding import Mesh
from jax.sharding import PartitionSpec as P

D = 4096
HEAD = 64
SP = ("sp_0", "sp_1")


EPS_GROUP = 0.00064
EPS_NORM = 1e-06
HIGHEST = lax.Precision.HIGHEST


def neutral_like(shard, identity):
    return jax.tree.map(
        lambda part, zero: jnp.zeros_like(part) + jnp.asarray(zero, part.dtype), shard, identity
    )


def carried_in(shard, axes, combine, identity):
    before = start = neutral_like(shard, identity)
    so_far = shard
    for axis in reversed(axes):
        size, mine = (lax.axis_size(axis), lax.axis_index(axis))
        pieces = jax.tree.map(
            lambda part, kind: lax.all_gather(part.astype(kind), axis),
            so_far,
            (jnp.bfloat16, jnp.bfloat16),
        )
        inside, so_far = (start, start)
        for k in range(size):
            passed = k < mine
            so_far = combine(
                so_far, jax.tree.map(lambda part, own: part[k].astype(own.dtype), pieces, shard)
            )
            inside = jax.tree.map(lambda new, old: jnp.where(passed, new, old), so_far, inside)
        before = combine(inside, before)
    return before


def from_everyone(shard, axis):
    size = lax.axis_size(axis)
    return lax.all_to_all(
        jnp.broadcast_to(shard[None], (size, *shard.shape)), axis, 0, 0, tiled=True
    )


def joined_along(pieces, dim):
    dims = list(pieces.shape[1:])
    dims[dim] *= pieces.shape[0]
    return jnp.moveaxis(pieces, 0, dim).reshape(dims)


def gather_directly(shard, axis, dim):
    pieces = from_everyone(shard, axis)
    return joined_along(pieces, dim)


def of_everyone(shard, axis):
    everything = from_everyone(shard, axis)
    return jnp.sum(everything, axis=0)


def split_up(shard, dim, size):
    before, after = (shard.shape[:dim], shard.shape[dim + 1 :])
    return jnp.moveaxis(shard.reshape(*before, size, -1, *after), dim, 0)


def sent_and_summed(shard, axis, dim):
    size = lax.axis_size(axis)
    pieces = lax.all_to_all(split_up(shard, dim, size), axis, 0, 0, tiled=True)
    return jnp.sum(pieces.astype(jnp.float32), axis=0)


def exact_einsum(pattern, first_op, second_op):
    return jnp.einsum(pattern, first_op, second_op, precision=HIGHEST)


F32 = jnp.float32
BF16 = jnp.bfloat16
CHUNK = 64


def iota2(shape, dim):
    return lax.broadcasted_iota(jnp.int32, shape, dim)


def halves(x):
    hi = x.astype(BF16)
    return hi, (x - hi.astype(F32)).astype(BF16)


def dot_dims(a, b, dims):
    return lax.dot_general(a, b, (dims, ((), ())), preferred_element_type=F32)


NN = ((1,), (0,))
NT = ((1,), (1,))
TN = ((0,), (0,))


def both_rows(x):
    hi, lo = halves(x)
    return jnp.concatenate([hi, lo], axis=0)


def left_split(a, b, dims=NN):
    rows = a.shape[0]
    full = dot_dims(both_rows(a), b, dims)
    return full[:rows] + full[rows:]


def two_split(a, b_hi, b_lo, dims=NN):
    rows = a.shape[0]
    hi, lo = halves(a)
    full = dot_dims(jnp.concatenate([hi, lo], axis=0), b_hi, dims)
    return full[:rows] + full[rows:] + dot_dims(hi, b_lo, dims)


def block_diag(x, mask):
    return jnp.concatenate([x] * (mask.shape[0] // x.shape[0]), axis=0) * mask


def block_dot(a, b, mask, dims=NN):
    b_hi, b_lo = halves(b)
    return two_split(a, block_diag(b_hi, mask), block_diag(b_lo, mask), dims)


def mix_body(r_ref, k_ref, v_ref, d_ref, b_ref, rd_ref, th_ref, ma_ref):
    tokens, width = r_ref.shape
    n = tokens // CHUNK
    row = iota2((width, width), 0)
    col = iota2((width, width), 1)
    same = (row // CHUNK) == (col // CHUNK)
    mask = same.astype(F32).astype(BF16)
    diag = row == col
    pos_t = iota2((CHUNK, width), 0)
    pos_s = iota2((CHUNK, width), 1) % CHUNK
    strict = pos_s < pos_t
    causal = pos_s <= pos_t
    eye_cat = (pos_s == pos_t).astype(F32)
    tri = (iota2((CHUNK, CHUNK), 1) <= iota2((CHUNK, CHUNK), 0)).astype(F32).astype(BF16)
    st = []
    for c in range(n):
        rows = pl.ds(c * CHUNK, CHUNK)
        recept = r_ref[rows, :].astype(F32)
        keyvec = k_ref[rows, :].astype(F32)
        val = v_ref[rows, :]
        logdec = (-0.6065306597126334) / (1.0 + jnp.exp(-d_ref[rows, :].astype(F32)))
        rate = 1.0 / (1.0 + jnp.exp(-b_ref[rows, :].astype(F32)))
        sums = left_split(keyvec * keyvec, mask)
        unit = keyvec * lax.rsqrt(1.0 + sums)
        corr = unit * rate
        ld_hi, ld_lo = halves(logdec)
        cum_in = dot_dims(tri, ld_hi, NN) + dot_dims(tri, ld_lo, NN)
        cum_ex = cum_in - logdec
        cum_end = cum_in[CHUNK - 1 : CHUNK, :]
        growth = jnp.exp(-cum_in)
        tail = jnp.exp(cum_end - cum_in)
        r_s = recept * jnp.exp(cum_in)
        u_s = unit * jnp.exp(cum_ex)
        st.append(dict(val=val, r_s=r_s, u_s=u_s, k_s=keyvec * growth, c_s=corr * growth,
                       c_tail=corr * tail, k_tail=keyvec * tail, keep=jnp.exp(cum_end)))
    for q in st:
        ur = jnp.concatenate([q["u_s"], q["r_s"]], axis=0)
        g_k = block_dot(ur, q["k_s"], mask, NT)
        g_c = block_dot(ur, q["c_s"], mask, NT)
        q["key_pull"] = jnp.where(strict, g_k[:CHUNK], 0.0)
        q["key_read"] = jnp.where(causal, g_k[CHUNK:], 0.0)
        q["low"] = jnp.where(strict, g_c[:CHUNK], 0.0)
        q["corr_read"] = jnp.where(causal, g_c[CHUNK:], 0.0)
        first = ((pos_t // 2) == (pos_s // 2)) & (pos_s < pos_t)
        q["x"] = eye_cat - jnp.where(first, q["low"], 0.0)
    size = 2
    while size < CHUNK:
        level = ((pos_t // (2 * size)) == (pos_s // (2 * size))) & ((pos_t // size) > (pos_s // size))
        for q in st:
            q["t"] = block_dot(q["x"], jnp.where(level, q["low"], 0.0), mask)
        for q in st:
            q["x"] = q["x"] - block_dot(q["t"], q["x"], mask)
        size *= 2
    for q in st:
        rl = left_split(jnp.concatenate([q["key_pull"], q["key_read"]], axis=0),
                        block_diag(q["val"], mask))
        q["right"], q["read"] = rl[:CHUNK], rl[CHUNK:]
    for q in st:
        q["pulled"] = block_dot(q["x"], q["right"], mask)
        q["reach"] = block_dot(q["x"], q["u_s"], mask)
    for q in st:
        q["read"] = q["read"] - block_dot(q["corr_read"], q["pulled"], mask)
        q["start"] = q["r_s"] - block_dot(q["corr_read"], q["reach"], mask)
        c_hi, c_lo = halves(q["c_tail"])
        k_hi, k_lo = halves(q["k_tail"])
        rh, rl_ = halves(q["reach"])
        full = (dot_dims(jnp.concatenate([rh, rl_, rh], axis=0),
                         jnp.concatenate([c_hi, c_hi, c_lo], axis=0), TN))
        q["map"] = jnp.where(same, jnp.where(diag, q["keep"], 0.0) - full, 0.0)
        ph, pl_ = halves(-q["pulled"])
        full = dot_dims(jnp.concatenate([q["val"], q["val"]], axis=0),
                        jnp.concatenate([k_hi, k_lo], axis=0), TN)
        full = full + dot_dims(jnp.concatenate([ph, pl_, ph], axis=0),
                               jnp.concatenate([c_hi, c_hi, c_lo], axis=0), TN)
        full = jnp.where(same, full, 0.0)
        q["add"] = sum(full[g * CHUNK : (g + 1) * CHUNK] for g in range(1, width // CHUNK)) + full[:CHUNK]
    ps = None
    for c, q in enumerate(st):
        rows = pl.ds(c * CHUNK, CHUNK)
        if c == 0:
            rd_ref[rows, :] = q["read"]
            th_ref[rows, :] = q["start"]
            m = q["map"]
            p = sum(m[g * CHUNK : (g + 1) * CHUNK] for g in range(1, width // CHUNK)) + m[:CHUNK]
            ps = jnp.concatenate([p, q["add"]], axis=0)
        else:
            th_ref[rows, :] = block_dot(q["start"], ps[:CHUNK], mask, NT)
            rd_ref[rows, :] = q["read"] + block_dot(q["start"], ps[CHUNK:], mask, NT)
            m_hi, m_lo = halves(q["map"])
            ps = two_split(ps, m_hi, m_lo)
            ps = jnp.concatenate([ps[:CHUNK], ps[CHUNK:] + q["add"]], axis=0)
    ma_ref[...] = ps


def mix_local(r, k, v, d, b):
    t, w = r.shape
    return pl.pallas_call(
        mix_body,
        out_shape=(
            jax.ShapeDtypeStruct((t, w), F32),
            jax.ShapeDtypeStruct((t, w), F32),
            jax.ShapeDtypeStruct((2 * CHUNK, w), F32),
        ),
        in_specs=[pl.BlockSpec(memory_space=pltpu.VMEM)] * 5,
        out_specs=(pl.BlockSpec(memory_space=pltpu.VMEM),) * 3,
        compiler_params=pltpu.CompilerParams(vmem_limit_bytes=48 * 1024 * 1024),
        name="mix_local",
    )(r, k, v, d, b)


def time_mix(
    receptance, key_vectors, value_vectors, decay_logits, rate_logits, gate_logits, group_gain
):
    tokens_here, channels = receptance.shape
    heads_here = channels // HEAD
    reads, through, ends = mix_local(
        receptance, key_vectors, value_vectors, decay_logits, rate_logits
    )
    eye_heads = jnp.broadcast_to(jnp.eye(HEAD, dtype=jnp.float32), (heads_here, HEAD, HEAD))
    zero_heads = jnp.zeros((heads_here, HEAD, HEAD), jnp.float32)
    device_map = jnp.swapaxes(ends[:HEAD].reshape(HEAD, heads_here, HEAD), 0, 1)
    device_add = jnp.swapaxes(ends[HEAD:].reshape(HEAD, heads_here, HEAD), 0, 1)

    def compose(earlier, following):
        return (
            exact_einsum("hij,hjl->hil", earlier[0], following[0]),
            exact_einsum("hij,hjl->hil", earlier[1], following[0]) + following[1],
        )

    prefix = carried_in((device_map, device_add), SP, compose, (eye_heads, zero_heads))
    incoming = prefix[1]
    head_shape = (tokens_here, heads_here, HEAD)
    state_read = reads.reshape(head_shape) + exact_einsum(
        "thj,hij->thi", through.reshape(head_shape), incoming
    )
    centred = state_read - jnp.mean(state_read, axis=-1, keepdims=True)
    scaled = centred * lax.rsqrt(jnp.mean(centred * centred, axis=-1, keepdims=True) + EPS_GROUP)
    gated_out = (
        scaled.reshape(tokens_here, channels)
        * group_gain[None, :]
        * jax.nn.sigmoid(gate_logits.astype(jnp.float32))
    )
    return gated_out.astype(jnp.bfloat16)


def local(
    receptance,
    key_vectors,
    value_vectors,
    decay_logits,
    rate_logits,
    gate_logits,
    group_gain,
    residual,
    mixer_out,
    norm_gain,
    expert_ids,
    route_weight,
    expert_gate,
    expert_up,
    expert_down,
):
    mixed_rows = time_mix(
        receptance, key_vectors, value_vectors, decay_logits, rate_logits, gate_logits, group_gain
    )
    tokens_here, features = residual.shape
    projected = jnp.dot(
        gather_directly(mixed_rows, "tp", 1), mixer_out, preferred_element_type=jnp.float32
    )
    midway = (residual.astype(jnp.float32) + projected).astype(jnp.bfloat16)
    midway_f = midway.astype(jnp.float32)
    squares = of_everyone(jnp.sum(midway_f * midway_f, axis=1), "tp")
    inv_rms = lax.rsqrt(squares / D + EPS_NORM)
    normed = (midway_f * norm_gain[None, :] * inv_rms[:, None]).astype(jnp.bfloat16)
    routes = expert_ids.shape[1]
    experts_all = lax.axis_size(SP) * expert_gate.shape[0]
    capacity = 2 * tokens_here * routes // experts_all
    flat_ids = expert_ids.reshape(-1)
    onehot = (flat_ids[:, None] == jnp.arange(experts_all, dtype=jnp.int32)[None, :]).astype(
        jnp.int32
    )
    earlier_count = jnp.sum((jnp.cumsum(onehot, axis=0) - onehot) * onehot, axis=1)
    slot_of = flat_ids * capacity + earlier_count
    owner_token = jnp.arange(tokens_here * routes, dtype=jnp.int32) // routes
    slot_table = (
        jnp.full((experts_all * capacity,), tokens_here, jnp.int32).at[slot_of].set(owner_token)
    )
    padded = jnp.concatenate([normed, jnp.zeros((1, features), jnp.bfloat16)], axis=0)
    outgoing = padded[slot_table].reshape(experts_all, capacity, features)
    arrived = lax.all_to_all(outgoing, SP, split_axis=0, concat_axis=0, tiled=True)
    arrived_rows = arrived.reshape(-1, features)
    paired = jnp.concatenate([expert_gate[0], expert_up[0]], axis=1)
    gate_up = sent_and_summed(
        jnp.dot(arrived_rows, paired, preferred_element_type=jnp.float32).astype(jnp.bfloat16),
        "tp",
        0,
    )
    half_width = paired.shape[1] // 2
    hidden = (jax.nn.silu(gate_up[:, :half_width]) * gate_up[:, half_width:]).astype(jnp.bfloat16)
    expert_res = jnp.dot(
        gather_directly(hidden, "tp", 0), expert_down[0], preferred_element_type=jnp.float32
    )
    returned = lax.all_to_all(
        expert_res.astype(jnp.bfloat16).reshape(-1, capacity, features),
        SP,
        split_axis=0,
        concat_axis=0,
        tiled=True,
    )
    picked = (
        returned.reshape(-1, features)[slot_of]
        .astype(jnp.float32)
        .reshape(tokens_here, routes, features)
    )
    routed_sum = jnp.sum(picked * route_weight[:, :, None], axis=1)
    return (midway_f + routed_sum).astype(jnp.bfloat16)


def solution(mesh):
    torus = Mesh(mesh.devices.reshape(16, 2, mesh.shape["tp"]), ("sp_0", "sp_1", "tp"))
    return jax.shard_map(
        local,
        mesh=torus,
        in_specs=(
            P(SP, "tp"),
            P(SP, "tp"),
            P(SP, "tp"),
            P(SP, "tp"),
            P(SP, "tp"),
            P(SP, "tp"),
            P("tp"),
            P(SP, "tp"),
            P(None, "tp"),
            P("tp"),
            P(SP, None),
            P(SP, None),
            P(SP, "tp", None),
            P(SP, "tp", None),
            P(SP, None, "tp"),
        ),
        out_specs=P(SP, "tp"),
        check_vma=False,
    )
```

```python
import functools
import jax
import jax.numpy as jnp
from jax import lax
from jax.experimental import pallas as pl
from jax.experimental.pallas import tpu as pltpu
from jax.sharding import Mesh
from jax.sharding import PartitionSpec as P

D = 4096
HEAD = 64
SP = ("z", "c")
TP = ("y", "x")


EPS_GROUP = 0.00064
EPS_NORM = 1e-06


def from_everyone(shard, axis):
    size = lax.axis_size(axis)
    return lax.all_to_all(
        jnp.broadcast_to(shard[None], (size, *shard.shape)), axis, 0, 0, tiled=True
    )


def joined_along(pieces, dim):
    dims = list(pieces.shape[1:])
    dims[dim] *= pieces.shape[0]
    return jnp.moveaxis(pieces, 0, dim).reshape(dims)


def gather_directly(shard, axis, dim):
    pieces = from_everyone(shard, axis)
    return joined_along(pieces, dim)


def of_everyone(shard, axis):
    everything = from_everyone(shard, axis)
    return jnp.sum(everything, axis=0)


def split_up(shard, dim, size):
    before, after = (shard.shape[:dim], shard.shape[dim + 1 :])
    return jnp.moveaxis(shard.reshape(*before, size, -1, *after), dim, 0)


def sent_and_summed(shard, axis, dim):
    size = lax.axis_size(axis)
    pieces = lax.all_to_all(split_up(shard, dim, size), axis, 0, 0, tiled=True)
    return jnp.sum(pieces.astype(jnp.float32), axis=0)


F32 = jnp.float32
BF16 = jnp.bfloat16
CHUNK = 64


def iota2(shape, dim):
    return lax.broadcasted_iota(jnp.int32, shape, dim)


def halves(x):
    hi = x.astype(BF16)
    return hi, (x - hi.astype(F32)).astype(BF16)


def dot_dims(a, b, dims):
    return lax.dot_general(a, b, (dims, ((), ())), preferred_element_type=F32)


NN = ((1,), (0,))
NT = ((1,), (1,))
TN = ((0,), (0,))


def both_rows(x):
    hi, lo = halves(x)
    return jnp.concatenate([hi, lo], axis=0)


def left_split(a, b, dims=NN):
    rows = a.shape[0]
    full = dot_dims(both_rows(a), b, dims)
    return full[:rows] + full[rows:]


def two_split(a, b_hi, b_lo, dims=NN):
    rows = a.shape[0]
    hi, lo = halves(a)
    full = dot_dims(jnp.concatenate([hi, lo], axis=0), b_hi, dims)
    return full[:rows] + full[rows:] + dot_dims(hi, b_lo, dims)


def block_diag(x, mask):
    return jnp.concatenate([x] * (mask.shape[0] // x.shape[0]), axis=0) * mask


def block_dot(a, b, mask, dims=NN):
    b_hi, b_lo = halves(b)
    return two_split(a, block_diag(b_hi, mask), block_diag(b_lo, mask), dims)


def mix_body(r_ref, k_ref, v_ref, d_ref, b_ref, rd_ref, th_ref, ma_ref):
    tokens, width = r_ref.shape
    n = tokens // CHUNK
    row = iota2((width, width), 0)
    col = iota2((width, width), 1)
    same = (row // CHUNK) == (col // CHUNK)
    mask = same.astype(F32).astype(BF16)
    diag = row == col
    pos_t = iota2((CHUNK, width), 0)
    pos_s = iota2((CHUNK, width), 1) % CHUNK
    strict = pos_s < pos_t
    causal = pos_s <= pos_t
    eye_cat = (pos_s == pos_t).astype(F32)
    tri = (iota2((CHUNK, CHUNK), 1) <= iota2((CHUNK, CHUNK), 0)).astype(F32).astype(BF16)
    st = []
    for c in range(n):
        rows = pl.ds(c * CHUNK, CHUNK)
        recept = r_ref[rows, :].astype(F32)
        keyvec = k_ref[rows, :].astype(F32)
        val = v_ref[rows, :]
        logdec = (-0.6065306597126334) / (1.0 + jnp.exp(-d_ref[rows, :].astype(F32)))
        rate = 1.0 / (1.0 + jnp.exp(-b_ref[rows, :].astype(F32)))
        sums = left_split(keyvec * keyvec, mask)
        unit = keyvec * lax.rsqrt(1.0 + sums)
        corr = unit * rate
        ld_hi, ld_lo = halves(logdec)
        cum_in = dot_dims(tri, ld_hi, NN) + dot_dims(tri, ld_lo, NN)
        cum_ex = cum_in - logdec
        cum_end = cum_in[CHUNK - 1 : CHUNK, :]
        growth = jnp.exp(-cum_in)
        tail = jnp.exp(cum_end - cum_in)
        r_s = recept * jnp.exp(cum_in)
        u_s = unit * jnp.exp(cum_ex)
        st.append(dict(val=val, r_s=r_s, u_s=u_s, k_s=keyvec * growth, c_s=corr * growth,
                       c_tail=corr * tail, k_tail=keyvec * tail, keep=jnp.exp(cum_end)))
    for q in st:
        ur = jnp.concatenate([q["u_s"], q["r_s"]], axis=0)
        g_k = block_dot(ur, q["k_s"], mask, NT)
        g_c = block_dot(ur, q["c_s"], mask, NT)
        q["key_pull"] = jnp.where(strict, g_k[:CHUNK], 0.0)
        q["key_read"] = jnp.where(causal, g_k[CHUNK:], 0.0)
        q["low"] = jnp.where(strict, g_c[:CHUNK], 0.0)
        q["corr_read"] = jnp.where(causal, g_c[CHUNK:], 0.0)
        first = ((pos_t // 2) == (pos_s // 2)) & (pos_s < pos_t)
        q["x"] = eye_cat - jnp.where(first, q["low"], 0.0)
    size = 2
    while size < CHUNK:
        level = ((pos_t // (2 * size)) == (pos_s // (2 * size))) & ((pos_t // size) > (pos_s // size))
        for q in st:
            q["t"] = block_dot(q["x"], jnp.where(level, q["low"], 0.0), mask)
        for q in st:
            q["x"] = q["x"] - block_dot(q["t"], q["x"], mask)
        size *= 2
    for q in st:
        rl = left_split(jnp.concatenate([q["key_pull"], q["key_read"]], axis=0),
                        block_diag(q["val"], mask))
        q["right"], q["read"] = rl[:CHUNK], rl[CHUNK:]
    for q in st:
        q["pulled"] = block_dot(q["x"], q["right"], mask)
        q["reach"] = block_dot(q["x"], q["u_s"], mask)
    for q in st:
        q["read"] = q["read"] - block_dot(q["corr_read"], q["pulled"], mask)
        q["start"] = q["r_s"] - block_dot(q["corr_read"], q["reach"], mask)
        c_hi, c_lo = halves(q["c_tail"])
        k_hi, k_lo = halves(q["k_tail"])
        rh, rl_ = halves(q["reach"])
        full = (dot_dims(jnp.concatenate([rh, rl_, rh], axis=0),
                         jnp.concatenate([c_hi, c_hi, c_lo], axis=0), TN))
        q["map"] = jnp.where(same, jnp.where(diag, q["keep"], 0.0) - full, 0.0)
        ph, pl_ = halves(-q["pulled"])
        full = dot_dims(jnp.concatenate([q["val"], q["val"]], axis=0),
                        jnp.concatenate([k_hi, k_lo], axis=0), TN)
        full = full + dot_dims(jnp.concatenate([ph, pl_, ph], axis=0),
                               jnp.concatenate([c_hi, c_hi, c_lo], axis=0), TN)
        full = jnp.where(same, full, 0.0)
        q["add"] = sum(full[g * CHUNK : (g + 1) * CHUNK] for g in range(1, width // CHUNK)) + full[:CHUNK]
    ps = None
    for c, q in enumerate(st):
        rows = pl.ds(c * CHUNK, CHUNK)
        if c == 0:
            rd_ref[rows, :] = q["read"]
            th_ref[rows, :] = q["start"]
            m = q["map"]
            p = sum(m[g * CHUNK : (g + 1) * CHUNK] for g in range(1, width // CHUNK)) + m[:CHUNK]
            ps = jnp.concatenate([p, q["add"]], axis=0)
        else:
            th_ref[rows, :] = block_dot(q["start"], ps[:CHUNK], mask, NT)
            rd_ref[rows, :] = q["read"] + block_dot(q["start"], ps[CHUNK:], mask, NT)
            m_hi, m_lo = halves(q["map"])
            ps = two_split(ps, m_hi, m_lo)
            ps = jnp.concatenate([ps[:CHUNK], ps[CHUNK:] + q["add"]], axis=0)
    ma_ref[...] = ps


def mix_local(r, k, v, d, b):
    t, w = r.shape
    return pl.pallas_call(
        mix_body,
        out_shape=(
            jax.ShapeDtypeStruct((t, w), F32),
            jax.ShapeDtypeStruct((t, w), F32),
            jax.ShapeDtypeStruct((2 * CHUNK, w), F32),
        ),
        in_specs=[pl.BlockSpec(memory_space=pltpu.VMEM)] * 5,
        out_specs=(pl.BlockSpec(memory_space=pltpu.VMEM),) * 3,
        compiler_params=pltpu.CompilerParams(vmem_limit_bytes=48 * 1024 * 1024),
        name="mix_local",
    )(r, k, v, d, b)


MESH = pl.DeviceIdType.MESH


def ring_order(size):
    near = sorted(range(1, size), key=lambda k: (min(k, size - k), k))
    return near


def remote(src, dst, send, recv, **where):
    return pltpu.make_async_remote_copy(
        src_ref=src, dst_ref=dst, send_sem=send, recv_sem=recv, device_id=where, device_id_type=MESH
    )


def greet(targets):
    barrier = pltpu.get_barrier_semaphore()
    for where in targets:
        pl.semaphore_signal(barrier, inc=1, device_id=where, device_id_type=MESH)
    pl.semaphore_wait(barrier, len(targets))


def share_blocks(buf, send, recv, y, x, ny, nx, use):
    mine = y * nx + x
    half = buf.shape[1] // 2
    sent = []

    def view(slot, part):
        return buf.at[slot, pl.ds(part * half, half), :]

    def push(slot, part, **where):
        copy = remote(view(slot, part), view(slot, part), send.at[len(sent)], recv.at[part, slot], **where)
        copy.start()
        sent.append(copy)

    def arrived(slot, part):
        remote(view(slot, part), view(slot, part), send.at[0], recv.at[part, slot], x=x).wait_recv()

    xs, ys = ring_order(nx), ring_order(ny)
    for k in range(max(len(xs), len(ys))):
        if k < len(xs):
            push(mine, 0, x=lax.rem(x + xs[k], nx))
        if k < len(ys):
            push(mine, 1, y=lax.rem(y + ys[k], ny))
    for k in ys:
        push(mine, 0, y=lax.rem(y + k, ny))
    for k in xs:
        push(mine, 1, x=lax.rem(x + k, nx))
    use(mine, 0)
    use(mine, 1)
    for k in range(max(len(xs), len(ys))):
        if k < len(xs):
            slot = y * nx + lax.rem(x + nx - xs[k], nx)
            arrived(slot, 0)
            for j in ys:
                push(slot, 0, y=lax.rem(y + j, ny))
            use(slot, 0)
        if k < len(ys):
            slot = lax.rem(y + ny - ys[k], ny) * nx + x
            arrived(slot, 1)
            for j in xs:
                push(slot, 1, x=lax.rem(x + j, nx))
            use(slot, 1)
    for k in ys:
        slot = lax.rem(y + ny - k, ny) * nx + x
        arrived(slot, 0)
        use(slot, 0)
    for k in xs:
        slot = y * nx + lax.rem(x + nx - k, nx)
        arrived(slot, 1)
        use(slot, 1)
    for a in xs:
        for b in ys:
            for part, (j, k) in ((0, (b, a)), (1, (b, a))):
                slot = lax.rem(y + ny - j, ny) * nx + lax.rem(x + nx - k, nx)
                arrived(slot, part)
                use(slot, part)
    return sent


def exact_left(a, b, mask, dims=NN):
    b_hi, b_lo = halves(b)
    return dot_dims(a, block_diag(b_hi, mask), dims) + dot_dims(a, block_diag(b_lo, mask), dims)


def flow_body(nz, ny, nx, rd_ref, th_ref, ma_ref, gate_ref, gain_ref, res_ref, ngain_ref, w_ref,
              mid_ref, norm_ref,
              pair_out, pair_in, hop_out, hop_in, near_in, far_out, far_in, back_out, back_in,
              blocks, total, sq_out, sq_in,
              pair_s, hop_s, fin_s, back_s, ag_send, ag_recv, sq_send, sq_recv):
    z, c, y, x = (lax.axis_index(name) for name in ("z", "c", "y", "x"))
    steps = []
    d = 1
    while d < nz // 2:
        steps.append(d)
        d *= 2
    far = nz // 2 + 1
    xs, ys = ring_order(nx), ring_order(ny)
    who = [dict(c=1 - c)]
    offs = []
    for d in steps + [1, far]:
        for o in (d, nz - d):
            if o % nz and o not in offs:
                offs.append(o)
    who += [dict(z=lax.rem(z + o, nz)) for o in offs]
    plane = [(a, b) for a in range(ny) for b in range(nx) if (a, b) != (0, 0)]
    who += [dict(y=lax.rem(y + a, ny), x=lax.rem(x + b, nx)) for a, b in plane]
    greet(who)

    wide = ma_ref.shape[1]
    part = wide // 2
    ends = ma_ref[...]
    low, high = ends[:, :part], ends[:, part:]
    first = c == 0
    pair_out[...] = jnp.where(first, high, low).astype(BF16)
    swap = remote(pair_out, pair_in, pair_s.at[0], pair_s.at[1], c=1 - c)
    swap.start()
    mine = jnp.where(first, low, high)
    mask = ((iota2((part, part), 0) // CHUNK) == (iota2((part, part), 1) // CHUNK)).astype(F32).astype(BF16)
    swap.wait()
    peer = pair_in[...].astype(F32)
    early = jnp.where(first, mine, peer)
    late = jnp.where(first, peer, mine)

    def compose(before, after):
        moved = block_dot(before, after[:CHUNK], mask)
        return jnp.concatenate([moved[:CHUNK], moved[CHUNK:] + after[CHUNK:]], axis=0)

    cur = compose(early, late)
    for i, d in enumerate(steps):
        hop_out[i] = cur.astype(BF16)
        hop = remote(hop_out.at[i], hop_in.at[i], hop_s.at[0, i], hop_s.at[1, i], z=lax.rem(z + d, nz))
        hop.start()
        hop.wait()
        joined = compose(hop_in[i].astype(F32), cur)
        cur = jnp.where(z >= d, joined, cur)
    last = len(steps)
    hop_out[last] = cur.astype(BF16)
    far_out[...] = cur[CHUNK:].astype(BF16)
    far_copy = remote(far_out, far_in, fin_s.at[0], fin_s.at[1], z=lax.rem(z + far, nz))
    far_copy.start()
    near_copy = remote(hop_out.at[last], near_in, fin_s.at[2], fin_s.at[3], z=lax.rem(z + 1, nz))
    near_copy.start()
    near_copy.wait()
    near = jnp.where(z >= 1, near_in[...].astype(F32), 0.0)
    far_copy.wait()
    far_add = jnp.where(z >= far, far_in[...].astype(F32), 0.0)
    start0 = block_dot(far_add, near[:CHUNK], mask) + near[CHUNK:]
    start1 = block_dot(start0, early[:CHUNK], mask) + early[CHUNK:]
    own = jnp.where(first, start0, start1)
    back_out[...] = jnp.where(first, start1, start0).astype(BF16)
    back = remote(back_out, back_in, back_s.at[0], back_s.at[1], c=1 - c)
    back.start()
    back.wait()
    other = back_in[...].astype(F32)
    incoming = jnp.concatenate([jnp.where(first, own, other), jnp.where(first, other, own)], axis=1)

    mask4 = ((iota2((wide, wide), 0) // CHUNK) == (iota2((wide, wide), 1) // CHUNK)).astype(F32).astype(BF16)
    read = rd_ref[...] + block_dot(th_ref[...], incoming, mask4, NT)
    centred = read - left_split(read, mask4) * (1.0 / CHUNK)
    spread = left_split(centred * centred, mask4) * (1.0 / CHUNK)
    gate = 1.0 / (1.0 + jnp.exp(-gate_ref[...].astype(F32)))
    mixed = centred * lax.rsqrt(spread + EPS_GROUP) * gain_ref[...] * gate
    tp = y * nx + x
    blocks[tp] = mixed.astype(BF16)
    total[...] = res_ref[...].astype(F32)
    half = blocks.shape[1] // 2

    def project(slot, part_no):
        rows = pl.ds(part_no * half, half)
        total[rows, :] += jnp.dot(blocks[slot, rows, :], w_ref[slot], preferred_element_type=F32)

    sent = share_blocks(blocks, ag_send, ag_recv, y, x, ny, nx, project)
    midway = total[...].astype(BF16)
    mid_ref[...] = midway
    mid_f = midway.astype(F32)
    s_hi, s_lo = halves(mid_f * mid_f)
    ones = jnp.ones((8, wide), BF16)
    sums = dot_dims(ones, s_hi, NT) + dot_dims(ones, s_lo, NT)
    sq_out[...] = sums
    pieces = []
    for i, (a, b) in enumerate(plane):
        copy = remote(sq_out, sq_in.at[i], sq_send.at[i], sq_recv.at[i],
                      y=lax.rem(y + a, ny), x=lax.rem(x + b, nx))
        copy.start()
        pieces.append(copy)
    for i, copy in enumerate(pieces):
        copy.wait_recv()
        sums = sums + sq_in[i]
    t_hi, t_lo = halves(sums)
    t_mid, t_lo = halves(sums - t_hi.astype(F32))
    eighth = jnp.full((8, wide), 0.125, BF16)
    squares = dot_dims(t_hi, eighth, TN) + dot_dims(t_mid, eighth, TN) + dot_dims(t_lo, eighth, TN)
    inv = lax.rsqrt(squares * (1.0 / (wide * ny * nx)) + EPS_NORM)
    norm_ref[...] = (mid_f * ngain_ref[...] * inv).astype(BF16)
    for copy in sent + pieces:
        copy.wait_send()


def flow(sizes, rd, th, ma, gate, gain, res, ngain, w):
    nz, ny, nx = sizes
    rows, wide = rd.shape
    part = wide // 2
    tp = ny * nx
    nstep = max(nz.bit_length() - 2, 0)
    dma = pltpu.SemaphoreType.DMA
    vm = pl.BlockSpec(memory_space=pltpu.VMEM)
    return pl.pallas_call(
        functools.partial(flow_body, nz, ny, nx),
        out_shape=(jax.ShapeDtypeStruct((rows, wide), BF16),) * 2,
        in_specs=[vm] * 8,
        out_specs=(vm, vm),
        scratch_shapes=[
            pltpu.VMEM((2 * CHUNK, part), BF16),
            pltpu.VMEM((2 * CHUNK, part), BF16),
            pltpu.VMEM((nstep + 1, 2 * CHUNK, part), BF16),
            pltpu.VMEM((max(nstep, 1), 2 * CHUNK, part), BF16),
            pltpu.VMEM((2 * CHUNK, part), BF16),
            pltpu.VMEM((CHUNK, part), BF16),
            pltpu.VMEM((CHUNK, part), BF16),
            pltpu.VMEM((CHUNK, part), BF16),
            pltpu.VMEM((CHUNK, part), BF16),
            pltpu.VMEM((tp, rows, wide), BF16),
            pltpu.VMEM((rows, wide), F32),
            pltpu.VMEM((8, rows), F32),
            pltpu.VMEM((tp - 1, 8, rows), F32),
            dma((2,)),
            dma((2, max(nstep, 1))),
            dma((4,)),
            dma((2,)),
            dma((2 * (tp - 1),)),
            dma((2, tp)),
            dma((tp - 1,)),
            dma((tp - 1,)),
        ],
        compiler_params=pltpu.CompilerParams(
            collective_id=0, has_side_effects=True, vmem_limit_bytes=32 * 1024 * 1024
        ),
        name="flow",
    )(rd, th, ma, gate, gain, res, ngain, w)


def local(
    receptance,
    key_vectors,
    value_vectors,
    decay_logits,
    rate_logits,
    gate_logits,
    group_gain,
    residual,
    mixer_out,
    norm_gain,
    expert_ids,
    route_weight,
    expert_gate,
    expert_up,
    expert_down,
):
    reads, through, ends = mix_local(
        receptance, key_vectors, value_vectors, decay_logits, rate_logits
    )
    tokens_here, features = residual.shape
    sizes = tuple(lax.axis_size(name) for name in ("z", "y", "x"))
    planes = sizes[1] * sizes[2]
    midway, normed = flow(
        sizes, reads, through, ends, gate_logits, group_gain[None], residual, norm_gain[None],
        mixer_out.reshape(planes, -1, features),
    )
    midway_f = midway.astype(jnp.float32)
    routes = expert_ids.shape[1]
    experts_all = lax.axis_size(SP) * expert_gate.shape[0]
    capacity = 2 * tokens_here * routes // experts_all
    flat_ids = expert_ids.reshape(-1)
    onehot = (flat_ids[:, None] == jnp.arange(experts_all, dtype=jnp.int32)[None, :]).astype(
        jnp.int32
    )
    earlier_count = jnp.sum((jnp.cumsum(onehot, axis=0) - onehot) * onehot, axis=1)
    slot_of = flat_ids * capacity + earlier_count
    owner_token = jnp.arange(tokens_here * routes, dtype=jnp.int32) // routes
    slot_table = (
        jnp.full((experts_all * capacity,), tokens_here, jnp.int32).at[slot_of].set(owner_token)
    )
    padded = jnp.concatenate([normed, jnp.zeros((1, features), jnp.bfloat16)], axis=0)
    outgoing = padded[slot_table].reshape(experts_all, capacity, features)
    arrived = lax.all_to_all(outgoing, SP, split_axis=0, concat_axis=0, tiled=True)
    arrived_rows = arrived.reshape(-1, features)
    paired = jnp.concatenate([expert_gate[0], expert_up[0]], axis=1)
    gate_up = sent_and_summed(
        jnp.dot(arrived_rows, paired, preferred_element_type=jnp.float32).astype(jnp.bfloat16),
        TP,
        0,
    )
    half_width = paired.shape[1] // 2
    hidden = (jax.nn.silu(gate_up[:, :half_width]) * gate_up[:, half_width:]).astype(jnp.bfloat16)
    expert_res = jnp.dot(
        gather_directly(hidden, TP, 0), expert_down[0], preferred_element_type=jnp.float32
    )
    returned = lax.all_to_all(
        expert_res.astype(jnp.bfloat16).reshape(-1, capacity, features),
        SP,
        split_axis=0,
        concat_axis=0,
        tiled=True,
    )
    picked = (
        returned.reshape(-1, features)[slot_of]
        .astype(jnp.float32)
        .reshape(tokens_here, routes, features)
    )
    routed_sum = jnp.sum(picked * route_weight[:, :, None], axis=1)
    return (midway_f + routed_sum).astype(jnp.bfloat16)


def solution(mesh):
    torus = Mesh(mesh.devices.reshape(16, 2, 4, 4), ("z", "c", "y", "x"))
    return jax.shard_map(
        local,
        mesh=torus,
        in_specs=(
            P(SP, TP),
            P(SP, TP),
            P(SP, TP),
            P(SP, TP),
            P(SP, TP),
            P(SP, TP),
            P(TP),
            P(SP, TP),
            P(None, TP),
            P(TP),
            P(SP, None),
            P(SP, None),
            P(SP, TP, None),
            P(SP, TP, None),
            P(SP, None, TP),
        ),
        out_specs=P(SP, TP),
        check_vma=False,
    )
```

```python
import functools
import jax
import jax.numpy as jnp
from jax import lax
from jax.experimental import pallas as pl
from jax.experimental.pallas import tpu as pltpu
from jax.sharding import Mesh
from jax.sharding import PartitionSpec as P

SP = ("z", "c")
TP = ("y", "x")


EPS_GROUP = 0.00064
EPS_NORM = 1e-06


F32 = jnp.float32
BF16 = jnp.bfloat16
CHUNK = 64


def iota2(shape, dim):
    return lax.broadcasted_iota(jnp.int32, shape, dim)


def halves(x):
    hi = x.astype(BF16)
    return hi, (x - hi.astype(F32)).astype(BF16)


def dot_dims(a, b, dims):
    return lax.dot_general(a, b, (dims, ((), ())), preferred_element_type=F32)


NN = ((1,), (0,))
NT = ((1,), (1,))
TN = ((0,), (0,))


def both_rows(x):
    hi, lo = halves(x)
    return jnp.concatenate([hi, lo], axis=0)


def left_split(a, b, dims=NN):
    rows = a.shape[0]
    full = dot_dims(both_rows(a), b, dims)
    return full[:rows] + full[rows:]


def two_split(a, b_hi, b_lo, dims=NN):
    rows = a.shape[0]
    hi, lo = halves(a)
    full = dot_dims(jnp.concatenate([hi, lo], axis=0), b_hi, dims)
    return full[:rows] + full[rows:] + dot_dims(hi, b_lo, dims)


def block_diag(x, mask):
    return jnp.concatenate([x] * (mask.shape[0] // x.shape[0]), axis=0) * mask


def block_dot(a, b, mask, dims=NN):
    b_hi, b_lo = halves(b)
    return two_split(a, block_diag(b_hi, mask), block_diag(b_lo, mask), dims)


def mix_body(r_ref, k_ref, v_ref, d_ref, b_ref, rd_ref, th_ref, ma_ref):
    tokens, width = r_ref.shape
    n = tokens // CHUNK
    row = iota2((width, width), 0)
    col = iota2((width, width), 1)
    same = (row // CHUNK) == (col // CHUNK)
    mask = same.astype(F32).astype(BF16)
    diag = row == col
    pos_t = iota2((CHUNK, width), 0)
    pos_s = iota2((CHUNK, width), 1) % CHUNK
    strict = pos_s < pos_t
    causal = pos_s <= pos_t
    eye_cat = (pos_s == pos_t).astype(F32)
    tri = (iota2((CHUNK, CHUNK), 1) <= iota2((CHUNK, CHUNK), 0)).astype(F32).astype(BF16)
    st = []
    for c in range(n):
        rows = pl.ds(c * CHUNK, CHUNK)
        recept = r_ref[rows, :].astype(F32)
        keyvec = k_ref[rows, :].astype(F32)
        val = v_ref[rows, :]
        logdec = (-0.6065306597126334) / (1.0 + jnp.exp(-d_ref[rows, :].astype(F32)))
        rate = 1.0 / (1.0 + jnp.exp(-b_ref[rows, :].astype(F32)))
        sums = left_split(keyvec * keyvec, mask)
        unit = keyvec * lax.rsqrt(1.0 + sums)
        corr = unit * rate
        ld_hi, ld_lo = halves(logdec)
        cum_in = dot_dims(tri, ld_hi, NN) + dot_dims(tri, ld_lo, NN)
        cum_ex = cum_in - logdec
        cum_end = cum_in[CHUNK - 1 : CHUNK, :]
        growth = jnp.exp(-cum_in)
        tail = jnp.exp(cum_end - cum_in)
        r_s = recept * jnp.exp(cum_in)
        u_s = unit * jnp.exp(cum_ex)
        st.append(dict(val=val, r_s=r_s, u_s=u_s, k_s=keyvec * growth, c_s=corr * growth,
                       c_tail=corr * tail, k_tail=keyvec * tail, keep=jnp.exp(cum_end)))
    for q in st:
        ur = jnp.concatenate([q["u_s"], q["r_s"]], axis=0)
        g_k = block_dot(ur, q["k_s"], mask, NT)
        g_c = block_dot(ur, q["c_s"], mask, NT)
        q["key_pull"] = jnp.where(strict, g_k[:CHUNK], 0.0)
        q["key_read"] = jnp.where(causal, g_k[CHUNK:], 0.0)
        q["low"] = jnp.where(strict, g_c[:CHUNK], 0.0)
        q["corr_read"] = jnp.where(causal, g_c[CHUNK:], 0.0)
        first = ((pos_t // 2) == (pos_s // 2)) & (pos_s < pos_t)
        q["x"] = eye_cat - jnp.where(first, q["low"], 0.0)
    size = 2
    while size < CHUNK:
        level = ((pos_t // (2 * size)) == (pos_s // (2 * size))) & ((pos_t // size) > (pos_s // size))
        for q in st:
            q["t"] = block_dot(q["x"], jnp.where(level, q["low"], 0.0), mask)
        for q in st:
            q["x"] = q["x"] - block_dot(q["t"], q["x"], mask)
        size *= 2
    for q in st:
        rl = left_split(jnp.concatenate([q["key_pull"], q["key_read"]], axis=0),
                        block_diag(q["val"], mask))
        q["right"], q["read"] = rl[:CHUNK], rl[CHUNK:]
    for q in st:
        q["pulled"] = block_dot(q["x"], q["right"], mask)
        q["reach"] = block_dot(q["x"], q["u_s"], mask)
    for q in st:
        q["read"] = q["read"] - block_dot(q["corr_read"], q["pulled"], mask)
        q["start"] = q["r_s"] - block_dot(q["corr_read"], q["reach"], mask)
        c_hi, c_lo = halves(q["c_tail"])
        k_hi, k_lo = halves(q["k_tail"])
        rh, rl_ = halves(q["reach"])
        full = (dot_dims(jnp.concatenate([rh, rl_, rh], axis=0),
                         jnp.concatenate([c_hi, c_hi, c_lo], axis=0), TN))
        q["map"] = jnp.where(same, jnp.where(diag, q["keep"], 0.0) - full, 0.0)
        ph, pl_ = halves(-q["pulled"])
        full = dot_dims(jnp.concatenate([q["val"], q["val"]], axis=0),
                        jnp.concatenate([k_hi, k_lo], axis=0), TN)
        full = full + dot_dims(jnp.concatenate([ph, pl_, ph], axis=0),
                               jnp.concatenate([c_hi, c_hi, c_lo], axis=0), TN)
        full = jnp.where(same, full, 0.0)
        q["add"] = sum(full[g * CHUNK : (g + 1) * CHUNK] for g in range(1, width // CHUNK)) + full[:CHUNK]
    ps = None
    for c, q in enumerate(st):
        rows = pl.ds(c * CHUNK, CHUNK)
        if c == 0:
            rd_ref[rows, :] = q["read"]
            th_ref[rows, :] = q["start"]
            m = q["map"]
            p = sum(m[g * CHUNK : (g + 1) * CHUNK] for g in range(1, width // CHUNK)) + m[:CHUNK]
            ps = jnp.concatenate([p, q["add"]], axis=0)
        else:
            th_ref[rows, :] = block_dot(q["start"], ps[:CHUNK], mask, NT)
            rd_ref[rows, :] = q["read"] + block_dot(q["start"], ps[CHUNK:], mask, NT)
            m_hi, m_lo = halves(q["map"])
            ps = two_split(ps, m_hi, m_lo)
            ps = jnp.concatenate([ps[:CHUNK], ps[CHUNK:] + q["add"]], axis=0)
    ma_ref[...] = ps


def mix_local(r, k, v, d, b):
    t, w = r.shape
    return pl.pallas_call(
        mix_body,
        out_shape=(
            jax.ShapeDtypeStruct((t, w), F32),
            jax.ShapeDtypeStruct((t, w), F32),
            jax.ShapeDtypeStruct((2 * CHUNK, w), F32),
        ),
        in_specs=[pl.BlockSpec(memory_space=pltpu.VMEM)] * 5,
        out_specs=(pl.BlockSpec(memory_space=pltpu.VMEM),) * 3,
        compiler_params=pltpu.CompilerParams(vmem_limit_bytes=48 * 1024 * 1024),
        name="mix_local",
    )(r, k, v, d, b)


MESH = pl.DeviceIdType.MESH


def ring_order(size):
    near = sorted(range(1, size), key=lambda k: (min(k, size - k), k))
    return near


def remote(src, dst, send, recv, **where):
    return pltpu.make_async_remote_copy(
        src_ref=src, dst_ref=dst, send_sem=send, recv_sem=recv, device_id=where, device_id_type=MESH
    )


def greet(targets):
    barrier = pltpu.get_barrier_semaphore()
    for where in targets:
        pl.semaphore_signal(barrier, inc=1, device_id=where, device_id_type=MESH)
    pl.semaphore_wait(barrier, len(targets))


def share_blocks(buf, send, recv, y, x, ny, nx, use):
    mine = y * nx + x
    half = buf.shape[1] // 2
    sent = []

    def view(slot, part):
        return buf.at[slot, pl.ds(part * half, half), :]

    def push(slot, part, **where):
        copy = remote(view(slot, part), view(slot, part), send.at[len(sent)], recv.at[part, slot], **where)
        copy.start()
        sent.append(copy)

    def arrived(slot, part):
        remote(view(slot, part), view(slot, part), send.at[0], recv.at[part, slot], x=x).wait_recv()

    xs, ys = ring_order(nx), ring_order(ny)
    for k in range(max(len(xs), len(ys))):
        if k < len(xs):
            push(mine, 0, x=lax.rem(x + xs[k], nx))
        if k < len(ys):
            push(mine, 1, y=lax.rem(y + ys[k], ny))
    for k in ys:
        push(mine, 0, y=lax.rem(y + k, ny))
    for k in xs:
        push(mine, 1, x=lax.rem(x + k, nx))
    use(mine, 0)
    use(mine, 1)
    for k in range(max(len(xs), len(ys))):
        if k < len(xs):
            slot = y * nx + lax.rem(x + nx - xs[k], nx)
            arrived(slot, 0)
            for j in ys:
                push(slot, 0, y=lax.rem(y + j, ny))
            use(slot, 0)
        if k < len(ys):
            slot = lax.rem(y + ny - ys[k], ny) * nx + x
            arrived(slot, 1)
            for j in xs:
                push(slot, 1, x=lax.rem(x + j, nx))
            use(slot, 1)
    for k in ys:
        slot = lax.rem(y + ny - k, ny) * nx + x
        arrived(slot, 0)
        use(slot, 0)
    for k in xs:
        slot = y * nx + lax.rem(x + nx - k, nx)
        arrived(slot, 1)
        use(slot, 1)
    for a in xs:
        for b in ys:
            for part, (j, k) in ((0, (b, a)), (1, (b, a))):
                slot = lax.rem(y + ny - j, ny) * nx + lax.rem(x + nx - k, nx)
                arrived(slot, part)
                use(slot, part)
    return sent


def exact_left(a, b, mask, dims=NN):
    b_hi, b_lo = halves(b)
    return dot_dims(a, block_diag(b_hi, mask), dims) + dot_dims(a, block_diag(b_lo, mask), dims)


def flow_body(nz, ny, nx, rd_ref, th_ref, ma_ref, gate_ref, gain_ref, res_ref, ngain_ref, w_ref,
              mid_ref, norm_ref,
              pair_out, pair_in, hop_out, hop_in, near_in, far_out, far_in, back_out, back_in,
              blocks, total, sq_out, sq_in,
              pair_s, hop_s, fin_s, back_s, ag_send, ag_recv, sq_send, sq_recv):
    z, c, y, x = (lax.axis_index(name) for name in ("z", "c", "y", "x"))
    steps = []
    d = 1
    while d < nz // 2:
        steps.append(d)
        d *= 2
    far = nz // 2 + 1
    xs, ys = ring_order(nx), ring_order(ny)
    who = [dict(c=1 - c)]
    offs = []
    for d in steps + [1, far]:
        for o in (d, nz - d):
            if o % nz and o not in offs:
                offs.append(o)
    who += [dict(z=lax.rem(z + o, nz)) for o in offs]
    plane = [(a, b) for a in range(ny) for b in range(nx) if (a, b) != (0, 0)]
    who += [dict(y=lax.rem(y + a, ny), x=lax.rem(x + b, nx)) for a, b in plane]
    greet(who)

    wide = ma_ref.shape[1]
    part = wide // 2
    ends = ma_ref[...]
    low, high = ends[:, :part], ends[:, part:]
    first = c == 0
    pair_out[...] = jnp.where(first, high, low).astype(BF16)
    swap = remote(pair_out, pair_in, pair_s.at[0], pair_s.at[1], c=1 - c)
    swap.start()
    mine = jnp.where(first, low, high)
    mask = ((iota2((part, part), 0) // CHUNK) == (iota2((part, part), 1) // CHUNK)).astype(F32).astype(BF16)
    swap.wait()
    peer = pair_in[...].astype(F32)
    early = jnp.where(first, mine, peer)
    late = jnp.where(first, peer, mine)

    def compose(before, after):
        moved = block_dot(before, after[:CHUNK], mask)
        return jnp.concatenate([moved[:CHUNK], moved[CHUNK:] + after[CHUNK:]], axis=0)

    cur = compose(early, late)
    for i, d in enumerate(steps):
        hop_out[i] = cur.astype(BF16)
        hop = remote(hop_out.at[i], hop_in.at[i], hop_s.at[0, i], hop_s.at[1, i], z=lax.rem(z + d, nz))
        hop.start()
        hop.wait()
        joined = compose(hop_in[i].astype(F32), cur)
        cur = jnp.where(z >= d, joined, cur)
    last = len(steps)
    hop_out[last] = cur.astype(BF16)
    far_out[...] = cur[CHUNK:].astype(BF16)
    far_copy = remote(far_out, far_in, fin_s.at[0], fin_s.at[1], z=lax.rem(z + far, nz))
    far_copy.start()
    near_copy = remote(hop_out.at[last], near_in, fin_s.at[2], fin_s.at[3], z=lax.rem(z + 1, nz))
    near_copy.start()
    near_copy.wait()
    near = jnp.where(z >= 1, near_in[...].astype(F32), 0.0)
    far_copy.wait()
    far_add = jnp.where(z >= far, far_in[...].astype(F32), 0.0)
    start0 = block_dot(far_add, near[:CHUNK], mask) + near[CHUNK:]
    start1 = block_dot(start0, early[:CHUNK], mask) + early[CHUNK:]
    own = jnp.where(first, start0, start1)
    back_out[...] = jnp.where(first, start1, start0).astype(BF16)
    back = remote(back_out, back_in, back_s.at[0], back_s.at[1], c=1 - c)
    back.start()
    back.wait()
    other = back_in[...].astype(F32)
    incoming = jnp.concatenate([jnp.where(first, own, other), jnp.where(first, other, own)], axis=1)

    mask4 = ((iota2((wide, wide), 0) // CHUNK) == (iota2((wide, wide), 1) // CHUNK)).astype(F32).astype(BF16)
    read = rd_ref[...] + block_dot(th_ref[...], incoming, mask4, NT)
    centred = read - left_split(read, mask4) * (1.0 / CHUNK)
    spread = left_split(centred * centred, mask4) * (1.0 / CHUNK)
    gate = 1.0 / (1.0 + jnp.exp(-gate_ref[...].astype(F32)))
    mixed = centred * lax.rsqrt(spread + EPS_GROUP) * gain_ref[...] * gate
    tp = y * nx + x
    blocks[tp] = mixed.astype(BF16)
    total[...] = res_ref[...].astype(F32)
    half = blocks.shape[1] // 2

    def project(slot, part_no):
        rows = pl.ds(part_no * half, half)
        total[rows, :] += jnp.dot(blocks[slot, rows, :], w_ref[slot], preferred_element_type=F32)

    sent = share_blocks(blocks, ag_send, ag_recv, y, x, ny, nx, project)
    midway = total[...].astype(BF16)
    mid_ref[...] = midway
    mid_f = midway.astype(F32)
    s_hi, s_lo = halves(mid_f * mid_f)
    ones = jnp.ones((8, wide), BF16)
    sums = dot_dims(ones, s_hi, NT) + dot_dims(ones, s_lo, NT)
    sq_out[...] = sums
    pieces = []
    for i, (a, b) in enumerate(plane):
        copy = remote(sq_out, sq_in.at[i], sq_send.at[i], sq_recv.at[i],
                      y=lax.rem(y + a, ny), x=lax.rem(x + b, nx))
        copy.start()
        pieces.append(copy)
    for i, copy in enumerate(pieces):
        copy.wait_recv()
        sums = sums + sq_in[i]
    t_hi, t_lo = halves(sums)
    t_mid, t_lo = halves(sums - t_hi.astype(F32))
    eighth = jnp.full((8, wide), 0.125, BF16)
    squares = dot_dims(t_hi, eighth, TN) + dot_dims(t_mid, eighth, TN) + dot_dims(t_lo, eighth, TN)
    inv = lax.rsqrt(squares * (1.0 / (wide * ny * nx)) + EPS_NORM)
    norm_ref[...] = (mid_f * ngain_ref[...] * inv).astype(BF16)
    for copy in sent + pieces:
        copy.wait_send()


def flow(sizes, rd, th, ma, gate, gain, res, ngain, w):
    nz, ny, nx = sizes
    rows, wide = rd.shape
    part = wide // 2
    tp = ny * nx
    nstep = max(nz.bit_length() - 2, 0)
    dma = pltpu.SemaphoreType.DMA
    vm = pl.BlockSpec(memory_space=pltpu.VMEM)
    return pl.pallas_call(
        functools.partial(flow_body, nz, ny, nx),
        out_shape=(jax.ShapeDtypeStruct((rows, wide), BF16),) * 2,
        in_specs=[vm] * 8,
        out_specs=(vm, vm),
        scratch_shapes=[
            pltpu.VMEM((2 * CHUNK, part), BF16),
            pltpu.VMEM((2 * CHUNK, part), BF16),
            pltpu.VMEM((nstep + 1, 2 * CHUNK, part), BF16),
            pltpu.VMEM((max(nstep, 1), 2 * CHUNK, part), BF16),
            pltpu.VMEM((2 * CHUNK, part), BF16),
            pltpu.VMEM((CHUNK, part), BF16),
            pltpu.VMEM((CHUNK, part), BF16),
            pltpu.VMEM((CHUNK, part), BF16),
            pltpu.VMEM((CHUNK, part), BF16),
            pltpu.VMEM((tp, rows, wide), BF16),
            pltpu.VMEM((rows, wide), F32),
            pltpu.VMEM((8, rows), F32),
            pltpu.VMEM((tp - 1, 8, rows), F32),
            dma((2,)),
            dma((2, max(nstep, 1))),
            dma((4,)),
            dma((2,)),
            dma((2 * (tp - 1),)),
            dma((2, tp)),
            dma((tp - 1,)),
            dma((tp - 1,)),
        ],
        compiler_params=pltpu.CompilerParams(
            collective_id=0, has_side_effects=True, vmem_limit_bytes=32 * 1024 * 1024
        ),
        name="flow",
    )(rd, th, ma, gate, gain, res, ngain, w)


def experts_body(nz, ny, nx, norm_ref, mid_ref, ids_ref, rw_ref, wg_ref, wu_ref, wd_ref, out_ref,
                 going, came, parts, from_x, from_y, sum_a, sum_b, last_a, last_b, hid, res, back,
                 pick_hi, pick_lo,
                 go_s, go_r, x_s, x_r, y_s, y_r, a_s, a_r, b_s, b_r, ag_send, ag_recv, re_s, re_r):
    z, c, y, x = (lax.axis_index(name) for name in ("z", "c", "y", "x"))
    me = 2 * z + c
    tp = y * nx + x
    tokens = norm_ref.shape[0]
    count, cap, _ = going.shape
    slots = count * cap
    ff = wg_ref.shape[1]
    hf = ff // 2
    xs, ys = ring_order(nx), ring_order(ny)
    zs = ring_order(nz)

    def core_of(flip):
        return 1 - c if flip else c

    barrier = pltpu.get_barrier_semaphore()
    who = [dict(c=1 - c)]
    who += [dict(z=lax.rem(z + o, nz), c=core_of(f)) for o in zs for f in (0, 1)]
    who += [dict(x=lax.rem(x + k, nx)) for k in xs] + [dict(y=lax.rem(y + k, ny)) for k in ys]
    for where in who:
        pl.semaphore_signal(barrier, inc=1, device_id=where, device_id_type=MESH)

    ids = ids_ref[...]
    id0, id1 = ids[:, 0:1], ids[:, 1:2]
    lane = iota2((tokens, 128), 1)
    hit = jnp.where((lane == id0) | (lane == id1), 1.0, 0.0).astype(BF16)
    tri = jnp.where(iota2((tokens, tokens), 1) < iota2((tokens, tokens), 0), 1.0, 0.0).astype(BF16)
    earlier = dot_dims(tri, hit, NN)

    def slot_of(one):
        rank = jnp.sum(jnp.where(lane == one, earlier, 0.0), axis=1, keepdims=True)
        return one * cap + rank.astype(jnp.int32)

    slot0, slot1 = slot_of(id0), slot_of(id1)
    spot = iota2((tokens, slots), 1)
    hot0, hot1 = spot == slot0, spot == slot1
    take = jnp.where(hot0 | hot1, 1.0, 0.0).astype(BF16)
    going[...] = dot_dims(take, norm_ref[...], TN).astype(BF16).reshape(going.shape)
    pl.semaphore_wait(barrier, len(who))

    sent = []

    def dispatch(zt, ct):
        e = 2 * zt + ct
        copy = remote(going.at[e], came.at[me], go_s.at[len(sent)], go_r.at[me], z=zt, c=ct)
        copy.start()
        sent.append(copy)

    came[me] = going[me]
    dispatch(z, 1 - c)
    for o in zs:
        for f in (0, 1):
            dispatch(lax.rem(z + o, nz), core_of(f))
    rw = rw_ref[...]
    weight = jnp.where(hot0, rw[:, 0:1], 0.0) + jnp.where(hot1, rw[:, 1:2], 0.0)
    w_hi, w_lo = halves(weight)
    pick_hi[...] = w_hi
    pick_lo[...] = w_lo

    def take_in(src):
        @pl.when(src != me)
        def _():
            remote(came.at[src], came.at[src], go_s.at[0], go_r.at[src], c=1 - c).wait_recv()

    def to_x(t):
        xt, yt = lax.rem(t, nx), lax.div(t, nx)
        return remote(parts.at[t, 0], from_x.at[x, yt], x_s.at[t], x_r.at[x, yt], x=xt)

    def to_y(t):
        xt, yt = lax.rem(t, nx), lax.div(t, nx)
        return remote(parts.at[t, 1], from_y.at[y, xt], y_s.at[t], y_r.at[y, xt], y=yt)

    def gate_up(k, carry):
        off = jnp.where(lax.rem(k, 2) == 1, lax.div(k + 1, 2), nz - lax.div(k, 2))
        t = lax.rem(z + off, nz)
        take_in(2 * t)
        take_in(2 * t + 1)
        rows = came[pl.ds(2 * t, 2)].reshape(2 * cap, came.shape[2])
        gate = jnp.dot(rows, wg_ref[...], preferred_element_type=F32).astype(BF16)
        up = jnp.dot(rows, wu_ref[...], preferred_element_type=F32).astype(BF16)
        parts[t, 0, :, :hf] = gate[:, :hf]
        parts[t, 0, :, hf:] = up[:, :hf]
        parts[t, 1, :, :hf] = gate[:, hf:]
        parts[t, 1, :, hf:] = up[:, hf:]

        @pl.when(lax.rem(t, nx) != x)
        def _():
            to_x(t).start()

        @pl.when(lax.div(t, nx) != y)
        def _():
            to_y(t).start()

        return carry

    lax.fori_loop(0, nz, gate_up, 0)

    def added_a(yb):
        acc = parts[yb * nx + x, 0].astype(F32)
        for k in xs:
            src = lax.rem(x + nx - k, nx)
            remote(from_x.at[src, yb], from_x.at[src, yb], x_s.at[0], x_r.at[src, yb], x=src).wait_recv()
            acc = acc + from_x[src, yb].astype(F32)
        return acc

    def added_b(xb):
        acc = parts[y * nx + xb, 1].astype(F32)
        for k in ys:
            src = lax.rem(y + ny - k, ny)
            remote(from_y.at[src, xb], from_y.at[src, xb], y_s.at[0], y_r.at[src, xb], y=src).wait_recv()
            acc = acc + from_y[src, xb].astype(F32)
        return acc

    second = []
    for k in range(max(len(xs), len(ys))):
        if k < len(ys):
            yb = lax.rem(y + ys[k], ny)
            sum_a[k] = added_a(yb).astype(BF16)
            copy = remote(sum_a.at[k], last_a.at[k], a_s.at[k], a_r.at[k], y=yb)
            copy.start()
            second.append(copy)
        if k < len(xs):
            xb = lax.rem(x + xs[k], nx)
            sum_b[k] = added_b(xb).astype(BF16)
            copy = remote(sum_b.at[k], last_b.at[k], b_s.at[k], b_r.at[k], x=xb)
            copy.start()
            second.append(copy)
    tot_a = added_a(y)
    tot_b = added_b(x)
    for copy in second:
        copy.wait_recv()
    for k in range(len(ys)):
        tot_a = tot_a + last_a[k].astype(F32)
    for k in range(len(xs)):
        tot_b = tot_b + last_b[k].astype(F32)

    def act(both):
        gate, up = both[:, :hf], both[:, hf:]
        return (gate / (1.0 + jnp.exp(-gate)) * up).astype(BF16)

    hid[tp, :, :hf] = act(tot_a)
    hid[tp, :, hf:] = act(tot_b)

    def give_back(slot, part):
        return remote(res.at[slot, part], back.at[me], re_s.at[slot, part], re_r.at[me], z=slot, c=part)

    def down(slot, part):
        rows = hid[slot, pl.ds(part * cap, cap), :]
        value = jnp.dot(rows, wd_ref[...], preferred_element_type=F32).astype(BF16)
        res[slot, part] = value
        own = jnp.logical_and(slot == z, c == part)

        @pl.when(own)
        def _():
            back[me] = value

        @pl.when(jnp.logical_not(own))
        def _():
            give_back(slot, part).start()

    shared = share_blocks(hid, ag_send, ag_recv, y, x, ny, nx, down)

    def collect(src, carry):
        @pl.when(src != me)
        def _():
            remote(back.at[src], back.at[src], re_s.at[0, 0], re_r.at[src], c=1 - c).wait_recv()

        return carry

    lax.fori_loop(0, count, collect, 0)
    rows = back[...].reshape(slots, back.shape[2])
    routed = dot_dims(pick_hi[...], rows, NN) + dot_dims(pick_lo[...], rows, NN)
    out_ref[...] = (mid_ref[...].astype(F32) + routed).astype(BF16)

    for copy in sent + second + shared:
        copy.wait_send()

    def drain(t, carry):
        @pl.when(lax.rem(t, nx) != x)
        def _():
            to_x(t).wait_send()

        @pl.when(lax.div(t, nx) != y)
        def _():
            to_y(t).wait_send()

        for part in (0, 1):
            @pl.when(jnp.logical_not(jnp.logical_and(t == z, c == part)))
            def _():
                give_back(t, part).wait_send()

        return carry

    lax.fori_loop(0, nz, drain, 0)


def experts(sizes, normed, midway, ids, weights, wg, wu, wd):
    nz, ny, nx = sizes
    tokens, wide = normed.shape
    ff = wg.shape[1]
    count = 2 * nz
    cap = 2 * tokens * ids.shape[1] // count
    tp = ny * nx
    rows = 2 * cap
    dma = pltpu.SemaphoreType.DMA
    vm = pl.BlockSpec(memory_space=pltpu.VMEM)
    return pl.pallas_call(
        functools.partial(experts_body, nz, ny, nx),
        out_shape=jax.ShapeDtypeStruct((tokens, wide), BF16),
        in_specs=[vm] * 7,
        out_specs=vm,
        scratch_shapes=[
            pltpu.VMEM((count, cap, wide), BF16),
            pltpu.VMEM((count, cap, wide), BF16),
            pltpu.VMEM((nz, 2, rows, ff), BF16),
            pltpu.VMEM((nx, ny, rows, ff), BF16),
            pltpu.VMEM((ny, nx, rows, ff), BF16),
            pltpu.VMEM((ny - 1, rows, ff), BF16),
            pltpu.VMEM((nx - 1, rows, ff), BF16),
            pltpu.VMEM((ny - 1, rows, ff), BF16),
            pltpu.VMEM((nx - 1, rows, ff), BF16),
            pltpu.VMEM((tp, rows, ff), BF16),
            pltpu.VMEM((nz, 2, cap, wide), BF16),
            pltpu.VMEM((count, cap, wide), BF16),
            pltpu.VMEM((tokens, count * cap), BF16),
            pltpu.VMEM((tokens, count * cap), BF16),
            dma((count - 1,)),
            dma((count,)),
            dma((nz,)),
            dma((nx, ny)),
            dma((nz,)),
            dma((ny, nx)),
            dma((ny - 1,)),
            dma((ny - 1,)),
            dma((nx - 1,)),
            dma((nx - 1,)),
            dma((2 * (tp - 1),)),
            dma((2, tp)),
            dma((nz, 2)),
            dma((count,)),
        ],
        compiler_params=pltpu.CompilerParams(
            collective_id=1, has_side_effects=True, vmem_limit_bytes=48 * 1024 * 1024
        ),
        name="experts",
    )(normed, midway, ids, weights, wg, wu, wd)


def local(
    receptance,
    key_vectors,
    value_vectors,
    decay_logits,
    rate_logits,
    gate_logits,
    group_gain,
    residual,
    mixer_out,
    norm_gain,
    expert_ids,
    route_weight,
    expert_gate,
    expert_up,
    expert_down,
):
    reads, through, ends = mix_local(
        receptance, key_vectors, value_vectors, decay_logits, rate_logits
    )
    tokens_here, features = residual.shape
    sizes = tuple(lax.axis_size(name) for name in ("z", "y", "x"))
    planes = sizes[1] * sizes[2]
    midway, normed = flow(
        sizes, reads, through, ends, gate_logits, group_gain[None], residual, norm_gain[None],
        mixer_out.reshape(planes, -1, features),
    )
    return experts(
        sizes, normed, midway, expert_ids, route_weight,
        expert_gate[0], expert_up[0], expert_down[0],
    )


def solution(mesh):
    torus = Mesh(mesh.devices.reshape(16, 2, 4, 4), ("z", "c", "y", "x"))
    return jax.shard_map(
        local,
        mesh=torus,
        in_specs=(
            P(SP, TP),
            P(SP, TP),
            P(SP, TP),
            P(SP, TP),
            P(SP, TP),
            P(SP, TP),
            P(TP),
            P(SP, TP),
            P(None, TP),
            P(TP),
            P(SP, None),
            P(SP, None),
            P(SP, TP, None),
            P(SP, TP, None),
            P(SP, None, TP),
        ),
        out_specs=P(SP, TP),
        check_vma=False,
    )
```

```python
import functools
import jax
import jax.numpy as jnp
from jax import lax
from jax.experimental import pallas as pl
from jax.experimental.pallas import tpu as pltpu
from jax.sharding import Mesh
from jax.sharding import PartitionSpec as P

SP = ("z", "c")
TP = ("y", "x")
F32 = jnp.float32
BF16 = jnp.bfloat16
CHUNK = 64


def iota2(shape, dim):
    return lax.broadcasted_iota(jnp.int32, shape, dim)


def halves(x):
    hi = x.astype(BF16)
    return hi, (x - hi.astype(F32)).astype(BF16)


def dot_dims(a, b, dims):
    return lax.dot_general(a, b, (dims, ((), ())), preferred_element_type=F32)


NN = ((1,), (0,))
NT = ((1,), (1,))
TN = ((0,), (0,))


def both_rows(x):
    hi, lo = halves(x)
    return jnp.concatenate([hi, lo], axis=0)


def left_split(a, b, dims=NN):
    rows = a.shape[0]
    full = dot_dims(both_rows(a), b, dims)
    return full[:rows] + full[rows:]


def two_split(a, b_hi, b_lo, dims=NN):
    rows = a.shape[0]
    hi, lo = halves(a)
    full = dot_dims(jnp.concatenate([hi, lo], axis=0), b_hi, dims)
    return full[:rows] + full[rows:] + dot_dims(hi, b_lo, dims)


def block_diag(x, mask):
    return jnp.concatenate([x] * (mask.shape[0] // x.shape[0]), axis=0) * mask


def block_dot(a, b, mask, dims=NN):
    b_hi, b_lo = halves(b)
    return two_split(a, block_diag(b_hi, mask), block_diag(b_lo, mask), dims)


def mix_body(r_ref, k_ref, v_ref, d_ref, b_ref, rd_ref, th_ref, ma_ref):
    tokens, width = r_ref.shape
    n = tokens // CHUNK
    row = iota2((width, width), 0)
    col = iota2((width, width), 1)
    same = (row // CHUNK) == (col // CHUNK)
    mask = same.astype(F32).astype(BF16)
    diag = row == col
    pos_t = iota2((CHUNK, width), 0)
    pos_s = iota2((CHUNK, width), 1) % CHUNK
    strict = pos_s < pos_t
    causal = pos_s <= pos_t
    eye_cat = (pos_s == pos_t).astype(F32)
    tri = (iota2((CHUNK, CHUNK), 1) <= iota2((CHUNK, CHUNK), 0)).astype(F32).astype(BF16)
    st = []
    for c in range(n):
        rows = pl.ds(c * CHUNK, CHUNK)
        recept = r_ref[rows, :].astype(F32)
        keyvec = k_ref[rows, :].astype(F32)
        val = v_ref[rows, :]
        logdec = (-0.6065306597126334) / (1.0 + jnp.exp(-d_ref[rows, :].astype(F32)))
        rate = 1.0 / (1.0 + jnp.exp(-b_ref[rows, :].astype(F32)))
        sums = left_split(keyvec * keyvec, mask)
        unit = keyvec * lax.rsqrt(1.0 + sums)
        corr = unit * rate
        ld_hi, ld_lo = halves(logdec)
        cum_in = dot_dims(tri, ld_hi, NN) + dot_dims(tri, ld_lo, NN)
        cum_ex = cum_in - logdec
        cum_end = cum_in[CHUNK - 1 : CHUNK, :]
        growth = jnp.exp(-cum_in)
        tail = jnp.exp(cum_end - cum_in)
        r_s = recept * jnp.exp(cum_in)
        u_s = unit * jnp.exp(cum_ex)
        st.append(dict(val=val, r_s=r_s, u_s=u_s, k_s=keyvec * growth, c_s=corr * growth,
                       c_tail=corr * tail, k_tail=keyvec * tail, keep=jnp.exp(cum_end)))
    for q in st:
        ur = jnp.concatenate([q["u_s"], q["r_s"]], axis=0)
        g_k = block_dot(ur, q["k_s"], mask, NT)
        g_c = block_dot(ur, q["c_s"], mask, NT)
        q["key_pull"] = jnp.where(strict, g_k[:CHUNK], 0.0)
        q["key_read"] = jnp.where(causal, g_k[CHUNK:], 0.0)
        q["low"] = jnp.where(strict, g_c[:CHUNK], 0.0)
        q["corr_read"] = jnp.where(causal, g_c[CHUNK:], 0.0)
        first = ((pos_t // 2) == (pos_s // 2)) & (pos_s < pos_t)
        q["x"] = eye_cat - jnp.where(first, q["low"], 0.0)
    size = 2
    while size < CHUNK:
        level = ((pos_t // (2 * size)) == (pos_s // (2 * size))) & ((pos_t // size) > (pos_s // size))
        for q in st:
            q["t"] = block_dot(q["x"], jnp.where(level, q["low"], 0.0), mask)
        for q in st:
            q["x"] = q["x"] - block_dot(q["t"], q["x"], mask)
        size *= 2
    for q in st:
        rl = left_split(jnp.concatenate([q["key_pull"], q["key_read"]], axis=0),
                        block_diag(q["val"], mask))
        q["right"], q["read"] = rl[:CHUNK], rl[CHUNK:]
    for q in st:
        q["pulled"] = block_dot(q["x"], q["right"], mask)
        q["reach"] = block_dot(q["x"], q["u_s"], mask)
    for q in st:
        q["read"] = q["read"] - block_dot(q["corr_read"], q["pulled"], mask)
        q["start"] = q["r_s"] - block_dot(q["corr_read"], q["reach"], mask)
        c_hi, c_lo = halves(q["c_tail"])
        k_hi, k_lo = halves(q["k_tail"])
        rh, rl_ = halves(q["reach"])
        full = (dot_dims(jnp.concatenate([rh, rl_, rh], axis=0),
                         jnp.concatenate([c_hi, c_hi, c_lo], axis=0), TN))
        q["map"] = jnp.where(same, jnp.where(diag, q["keep"], 0.0) - full, 0.0)
        ph, pl_ = halves(-q["pulled"])
        full = dot_dims(jnp.concatenate([q["val"], q["val"]], axis=0),
                        jnp.concatenate([k_hi, k_lo], axis=0), TN)
        full = full + dot_dims(jnp.concatenate([ph, pl_, ph], axis=0),
                               jnp.concatenate([c_hi, c_hi, c_lo], axis=0), TN)
        full = jnp.where(same, full, 0.0)
        q["add"] = sum(full[g * CHUNK : (g + 1) * CHUNK] for g in range(1, width // CHUNK)) + full[:CHUNK]
    ps = None
    for c, q in enumerate(st):
        rows = pl.ds(c * CHUNK, CHUNK)
        if c == 0:
            rd_ref[rows, :] = q["read"]
            th_ref[rows, :] = q["start"]
            m = q["map"]
            p = sum(m[g * CHUNK : (g + 1) * CHUNK] for g in range(1, width // CHUNK)) + m[:CHUNK]
            ps = jnp.concatenate([p, q["add"]], axis=0)
        else:
            th_ref[rows, :] = block_dot(q["start"], ps[:CHUNK], mask, NT)
            rd_ref[rows, :] = q["read"] + block_dot(q["start"], ps[CHUNK:], mask, NT)
            m_hi, m_lo = halves(q["map"])
            ps = two_split(ps, m_hi, m_lo)
            ps = jnp.concatenate([ps[:CHUNK], ps[CHUNK:] + q["add"]], axis=0)
    ma_ref[...] = ps


MESH = pl.DeviceIdType.MESH
EPS_GROUP = 0.00064
EPS_NORM = 1e-06


def ring_order(size):
    near = sorted(range(1, size), key=lambda k: (min(k, size - k), k))
    return near


def remote(src, dst, send, recv, **where):
    return pltpu.make_async_remote_copy(
        src_ref=src, dst_ref=dst, send_sem=send, recv_sem=recv, device_id=where, device_id_type=MESH
    )


def share_blocks(buf, send, recv, y, x, ny, nx, use):
    mine = y * nx + x
    half = buf.shape[1] // 2
    sent = []

    def view(slot, part):
        return buf.at[slot, pl.ds(part * half, half), :]

    def push(slot, part, **where):
        copy = remote(view(slot, part), view(slot, part), send.at[len(sent)], recv.at[part, slot], **where)
        copy.start()
        sent.append(copy)

    def arrived(slot, part):
        remote(view(slot, part), view(slot, part), send.at[0], recv.at[part, slot], x=x).wait_recv()

    xs, ys = ring_order(nx), ring_order(ny)
    for k in range(max(len(xs), len(ys))):
        if k < len(xs):
            push(mine, 0, x=lax.rem(x + xs[k], nx))
        if k < len(ys):
            push(mine, 1, y=lax.rem(y + ys[k], ny))
    for k in ys:
        push(mine, 0, y=lax.rem(y + k, ny))
    for k in xs:
        push(mine, 1, x=lax.rem(x + k, nx))
    use(mine, 0)
    use(mine, 1)
    for k in range(max(len(xs), len(ys))):
        if k < len(xs):
            slot = y * nx + lax.rem(x + nx - xs[k], nx)
            arrived(slot, 0)
            for j in ys:
                push(slot, 0, y=lax.rem(y + j, ny))
            use(slot, 0)
        if k < len(ys):
            slot = lax.rem(y + ny - ys[k], ny) * nx + x
            arrived(slot, 1)
            for j in xs:
                push(slot, 1, x=lax.rem(x + j, nx))
            use(slot, 1)
    for k in ys:
        slot = lax.rem(y + ny - k, ny) * nx + x
        arrived(slot, 0)
        use(slot, 0)
    for k in xs:
        slot = y * nx + lax.rem(x + nx - k, nx)
        arrived(slot, 1)
        use(slot, 1)
    for a in xs:
        for b in ys:
            for part, (j, k) in ((0, (b, a)), (1, (b, a))):
                slot = lax.rem(y + ny - j, ny) * nx + lax.rem(x + nx - k, nx)
                arrived(slot, part)
                use(slot, part)
    return sent


def exact_left(a, b, mask, dims=NN):
    b_hi, b_lo = halves(b)
    return dot_dims(a, block_diag(b_hi, mask), dims) + dot_dims(a, block_diag(b_lo, mask), dims)


def flow_body(nz, ny, nx, rd_ref, th_ref, ma_ref, gate_ref, gain_ref, res_ref, ngain_ref, w_ref,
              mid_ref, norm_ref,
              pair_out, pair_in, hop_out, hop_in, near_in, far_out, far_in, back_out, back_in,
              blocks, total, sq_out, sq_in,
              pair_s, hop_s, fin_s, back_s, ag_send, ag_recv, sq_send, sq_recv):
    z, c, y, x = (lax.axis_index(name) for name in ("z", "c", "y", "x"))
    steps = []
    d = 1
    while d < nz // 2:
        steps.append(d)
        d *= 2
    far = nz // 2 + 1
    xs, ys = ring_order(nx), ring_order(ny)
    plane = [(a, b) for a in range(ny) for b in range(nx) if (a, b) != (0, 0)]
    wide = ma_ref.shape[1]
    part = wide // 2
    ends = ma_ref[...]
    low, high = ends[:, :part], ends[:, part:]
    first = c == 0
    pair_out[...] = jnp.where(first, high, low).astype(BF16)
    swap = remote(pair_out, pair_in, pair_s.at[0], pair_s.at[1], c=1 - c)
    swap.start()
    mine = jnp.where(first, low, high)
    mask = ((iota2((part, part), 0) // CHUNK) == (iota2((part, part), 1) // CHUNK)).astype(F32).astype(BF16)
    with jax.named_scope("pair"):
        swap.wait()
    peer = pair_in[...].astype(F32)
    early = jnp.where(first, mine, peer)
    late = jnp.where(first, peer, mine)

    def compose(before, after):
        moved = block_dot(before, after[:CHUNK], mask)
        return jnp.concatenate([moved[:CHUNK], moved[CHUNK:] + after[CHUNK:]], axis=0)

    cur = compose(early, late)
    for i, d in enumerate(steps):
        hop_out[i] = cur.astype(BF16)
        hop = remote(hop_out.at[i], hop_in.at[i], hop_s.at[0, i], hop_s.at[1, i], z=lax.rem(z + d, nz))
        hop.start()
        with jax.named_scope(f"hop{d}"):
            hop.wait()
        joined = compose(hop_in[i].astype(F32), cur)
        cur = jnp.where(z >= d, joined, cur)
    last = len(steps)
    hop_out[last] = cur.astype(BF16)
    far_out[...] = cur[CHUNK:].astype(BF16)
    far_copy = remote(far_out, far_in, fin_s.at[0], fin_s.at[1], z=lax.rem(z + far, nz))
    far_copy.start()
    near_copy = remote(hop_out.at[last], near_in, fin_s.at[2], fin_s.at[3], z=lax.rem(z + 1, nz))
    near_copy.start()
    with jax.named_scope("near"):
        near_copy.wait()
    near = jnp.where(z >= 1, near_in[...].astype(F32), 0.0)
    with jax.named_scope("far"):
        far_copy.wait()
    far_add = jnp.where(z >= far, far_in[...].astype(F32), 0.0)
    start0 = block_dot(far_add, near[:CHUNK], mask) + near[CHUNK:]
    start1 = block_dot(start0, early[:CHUNK], mask) + early[CHUNK:]
    own = jnp.where(first, start0, start1)
    back_out[...] = jnp.where(first, start1, start0).astype(BF16)
    back = remote(back_out, back_in, back_s.at[0], back_s.at[1], c=1 - c)
    back.start()
    with jax.named_scope("back"):
        back.wait()
    other = back_in[...].astype(F32)
    incoming = jnp.concatenate([jnp.where(first, own, other), jnp.where(first, other, own)], axis=1)

    mask4 = ((iota2((wide, wide), 0) // CHUNK) == (iota2((wide, wide), 1) // CHUNK)).astype(F32).astype(BF16)
    read = rd_ref[...] + block_dot(th_ref[...], incoming, mask4, NT)
    centred = read - left_split(read, mask4) * (1.0 / CHUNK)
    spread = left_split(centred * centred, mask4) * (1.0 / CHUNK)
    gate = 1.0 / (1.0 + jnp.exp(-gate_ref[...].astype(F32)))
    mixed = centred * lax.rsqrt(spread + EPS_GROUP) * gain_ref[...] * gate
    tp = y * nx + x
    blocks[tp] = mixed.astype(BF16)
    total[...] = res_ref[...].astype(F32)
    half = blocks.shape[1] // 2

    def project(slot, part_no):
        rows = pl.ds(part_no * half, half)
        total[rows, :] += jnp.dot(blocks[slot, rows, :], w_ref[slot], preferred_element_type=F32)

    with jax.named_scope("share"):
        sent = share_blocks(blocks, ag_send, ag_recv, y, x, ny, nx, project)
    midway = total[...].astype(BF16)
    mid_ref[...] = midway
    mid_f = midway.astype(F32)
    s_hi, s_lo = halves(mid_f * mid_f)
    ones = jnp.ones((8, wide), BF16)
    sums = dot_dims(ones, s_hi, NT) + dot_dims(ones, s_lo, NT)
    sq_out[...] = sums
    pieces = []
    for i, (a, b) in enumerate(plane):
        copy = remote(sq_out, sq_in.at[i], sq_send.at[i], sq_recv.at[i],
                      y=lax.rem(y + a, ny), x=lax.rem(x + b, nx))
        copy.start()
        pieces.append(copy)
    with jax.named_scope("squares"):
        for i, copy in enumerate(pieces):
            copy.wait_recv()
            sums = sums + sq_in[i]
    t_hi, t_lo = halves(sums)
    t_mid, t_lo = halves(sums - t_hi.astype(F32))
    eighth = jnp.full((8, wide), 0.125, BF16)
    squares = dot_dims(t_hi, eighth, TN) + dot_dims(t_mid, eighth, TN) + dot_dims(t_lo, eighth, TN)
    inv = lax.rsqrt(squares * (1.0 / (wide * ny * nx)) + EPS_NORM)
    norm_ref[...] = (mid_f * ngain_ref[...] * inv).astype(BF16)
    for copy in sent + pieces:
        copy.wait_send()


def experts_body(nz, ny, nx, norm_ref, mid_ref, ids_ref, rw_ref, wg_ref, wu_ref, wd_ref, out_ref,
                 going, came, parts, from_x, from_y, sum_a, sum_b, last_a, last_b, hid, res, back,
                 pick_hi, pick_lo,
                 go_s, go_r, x_s, x_r, y_s, y_r, a_s, a_r, b_s, b_r, ag_send, ag_recv, re_s, re_r):
    z, c, y, x = (lax.axis_index(name) for name in ("z", "c", "y", "x"))
    me = 2 * z + c
    tp = y * nx + x
    tokens = norm_ref.shape[0]
    count, cap, _ = going.shape
    slots = count * cap
    ff = wg_ref.shape[1]
    hf = ff // 2
    xs, ys = ring_order(nx), ring_order(ny)
    zs = ring_order(nz)

    def core_of(flip):
        return 1 - c if flip else c

    ids = ids_ref[...]
    id0, id1 = ids[:, 0:1], ids[:, 1:2]
    lane = iota2((tokens, 128), 1)
    hit = jnp.where((lane == id0) | (lane == id1), 1.0, 0.0).astype(BF16)
    tri = jnp.where(iota2((tokens, tokens), 1) < iota2((tokens, tokens), 0), 1.0, 0.0).astype(BF16)
    earlier = dot_dims(tri, hit, NN)

    def slot_of(one):
        rank = jnp.sum(jnp.where(lane == one, earlier, 0.0), axis=1, keepdims=True)
        return one * cap + rank.astype(jnp.int32)

    with jax.named_scope("route"):
        slot0, slot1 = slot_of(id0), slot_of(id1)
    spot = iota2((tokens, slots), 1)
    hot0, hot1 = spot == slot0, spot == slot1
    take = jnp.where(hot0 | hot1, 1.0, 0.0).astype(BF16)
    going[...] = dot_dims(take, norm_ref[...], TN).astype(BF16).reshape(going.shape)

    sent = []

    def dispatch(zt, ct):
        e = 2 * zt + ct
        copy = remote(going.at[e], came.at[me], go_s.at[len(sent)], go_r.at[me], z=zt, c=ct)
        copy.start()
        sent.append(copy)

    came[me] = going[me]
    dispatch(z, 1 - c)
    for o in zs:
        for f in (0, 1):
            dispatch(lax.rem(z + o, nz), core_of(f))
    rw = rw_ref[...]
    weight = jnp.where(hot0, rw[:, 0:1], 0.0) + jnp.where(hot1, rw[:, 1:2], 0.0)
    w_hi, w_lo = halves(weight)
    pick_hi[...] = w_hi
    pick_lo[...] = w_lo

    def take_in(src):
        @pl.when(src != me)
        def _():
            remote(came.at[src], came.at[src], go_s.at[0], go_r.at[src], c=1 - c).wait_recv()

    def to_x(t):
        xt, yt = lax.rem(t, nx), lax.div(t, nx)
        return remote(parts.at[t, 0], from_x.at[x, yt], x_s.at[t], x_r.at[x, yt], x=xt)

    def to_y(t):
        xt, yt = lax.rem(t, nx), lax.div(t, nx)
        return remote(parts.at[t, 1], from_y.at[y, xt], y_s.at[t], y_r.at[y, xt], y=yt)

    def gate_up(k, carry):
        off = jnp.where(lax.rem(k, 2) == 1, lax.div(k + 1, 2), nz - lax.div(k, 2))
        t = lax.rem(z + off, nz)
        take_in(2 * t)
        take_in(2 * t + 1)
        rows = came[pl.ds(2 * t, 2)].reshape(2 * cap, came.shape[2])
        gate = jnp.dot(rows, wg_ref[...], preferred_element_type=F32).astype(BF16)
        up = jnp.dot(rows, wu_ref[...], preferred_element_type=F32).astype(BF16)
        parts[t, 0, :, :hf] = gate[:, :hf]
        parts[t, 0, :, hf:] = up[:, :hf]
        parts[t, 1, :, :hf] = gate[:, hf:]
        parts[t, 1, :, hf:] = up[:, hf:]

        @pl.when(lax.rem(t, nx) != x)
        def _():
            to_x(t).start()

        @pl.when(lax.div(t, nx) != y)
        def _():
            to_y(t).start()

        return carry

    with jax.named_scope("gateup"):
        lax.fori_loop(0, nz, gate_up, 0)

    def added_a(yb):
        acc = parts[yb * nx + x, 0].astype(F32)
        for k in xs:
            src = lax.rem(x + nx - k, nx)
            remote(from_x.at[src, yb], from_x.at[src, yb], x_s.at[0], x_r.at[src, yb], x=src).wait_recv()
            acc = acc + from_x[src, yb].astype(F32)
        return acc

    def added_b(xb):
        acc = parts[y * nx + xb, 1].astype(F32)
        for k in ys:
            src = lax.rem(y + ny - k, ny)
            remote(from_y.at[src, xb], from_y.at[src, xb], y_s.at[0], y_r.at[src, xb], y=src).wait_recv()
            acc = acc + from_y[src, xb].astype(F32)
        return acc

    second = []
    with jax.named_scope("second"):
        for k in range(max(len(xs), len(ys))):
            if k < len(ys):
                yb = lax.rem(y + ys[k], ny)
                sum_a[k] = added_a(yb).astype(BF16)
                copy = remote(sum_a.at[k], last_a.at[k], a_s.at[k], a_r.at[k], y=yb)
                copy.start()
                second.append(copy)
            if k < len(xs):
                xb = lax.rem(x + xs[k], nx)
                sum_b[k] = added_b(xb).astype(BF16)
                copy = remote(sum_b.at[k], last_b.at[k], b_s.at[k], b_r.at[k], x=xb)
                copy.start()
                second.append(copy)
    tot_a = added_a(y)
    tot_b = added_b(x)
    with jax.named_scope("last"):
        for copy in second:
            copy.wait_recv()
    for k in range(len(ys)):
        tot_a = tot_a + last_a[k].astype(F32)
    for k in range(len(xs)):
        tot_b = tot_b + last_b[k].astype(F32)

    def act(both):
        gate, up = both[:, :hf], both[:, hf:]
        return (gate / (1.0 + jnp.exp(-gate)) * up).astype(BF16)

    hid[tp, :, :hf] = act(tot_a)
    hid[tp, :, hf:] = act(tot_b)

    def give_back(slot, part):
        return remote(res.at[slot, part], back.at[me], re_s.at[slot, part], re_r.at[me], z=slot, c=part)

    def down(slot, part):
        rows = hid[slot, pl.ds(part * cap, cap), :]
        value = jnp.dot(rows, wd_ref[...], preferred_element_type=F32).astype(BF16)
        res[slot, part] = value
        own = jnp.logical_and(slot == z, c == part)

        @pl.when(own)
        def _():
            back[me] = value

        @pl.when(jnp.logical_not(own))
        def _():
            give_back(slot, part).start()

    with jax.named_scope("down"):
        shared = share_blocks(hid, ag_send, ag_recv, y, x, ny, nx, down)

    def collect(src, carry):
        @pl.when(src != me)
        def _():
            remote(back.at[src], back.at[src], re_s.at[0, 0], re_r.at[src], c=1 - c).wait_recv()

        return carry

    with jax.named_scope("collect"):
        lax.fori_loop(0, count, collect, 0)
    rows = back[...].reshape(slots, back.shape[2])
    routed = dot_dims(pick_hi[...], rows, NN) + dot_dims(pick_lo[...], rows, NN)
    out_ref[...] = (mid_ref[...].astype(F32) + routed).astype(BF16)

    for copy in sent + second + shared:
        copy.wait_send()

    def drain(t, carry):
        @pl.when(lax.rem(t, nx) != x)
        def _():
            to_x(t).wait_send()

        @pl.when(lax.div(t, nx) != y)
        def _():
            to_y(t).wait_send()

        for part in (0, 1):
            @pl.when(jnp.logical_not(jnp.logical_and(t == z, c == part)))
            def _():
                give_back(t, part).wait_send()

        return carry

    with jax.named_scope("drain"):
        lax.fori_loop(0, nz, drain, 0)

def layer_body(nz, ny, nx, r_hbm, k_hbm, v_hbm, d_hbm, b_hbm, gate_hbm, gain_ref, res_hbm, w_hbm, ngain_ref,
               ids_ref, rw_ref, wg_hbm, wu_hbm, wd_hbm, out_ref,
               r_ref, k_ref, v_ref, d_ref, b_ref, gate_ref, res_ref, w_ref, wg_ref, wu_ref, wd_ref,
               rd_ref, th_ref, ma_ref, mid_ref, norm_ref, load_s, *rest):
    z, c, y, x = (lax.axis_index(name) for name in ("z", "c", "y", "x"))
    loads = [
        pltpu.make_async_copy(src, dst, load_s.at[i])
        for i, (src, dst) in enumerate((
            (d_hbm, d_ref), (k_hbm, k_ref), (b_hbm, b_ref), (r_hbm, r_ref), (v_hbm, v_ref),
            (gate_hbm, gate_ref), (res_hbm, res_ref), (w_hbm, w_ref),
            (wg_hbm, wg_ref), (wu_hbm, wu_ref), (wd_hbm, wd_ref),
        ))
    ]
    for copy in loads:
        copy.start()
    barrier = pltpu.get_barrier_semaphore()
    plane = [(a, b) for a in range(ny) for b in range(nx) if (a, b) != (0, 0)]
    who = [dict(c=1 - c)]
    who += [dict(z=lax.rem(z + o, nz), c=1 - c if f else c) for o in ring_order(nz) for f in (0, 1)]
    who += [dict(y=lax.rem(y + a, ny), x=lax.rem(x + b, nx)) for a, b in plane]
    for where in who:
        pl.semaphore_signal(barrier, inc=1, device_id=where, device_id_type=MESH)
    for copy in loads[:5]:
        copy.wait()
    with jax.named_scope("mix"):
        mix_body(r_ref, k_ref, v_ref, d_ref, b_ref, rd_ref, th_ref, ma_ref)
    with jax.named_scope("meet"):
        pl.semaphore_wait(barrier, len(who))
        for copy in loads[5:]:
            copy.wait()
    flow_body(nz, ny, nx, rd_ref, th_ref, ma_ref, gate_ref, gain_ref, res_ref, ngain_ref, w_ref,
              mid_ref, norm_ref, *rest[:FLOW_SCRATCH])
    experts_body(nz, ny, nx, norm_ref, mid_ref, ids_ref, rw_ref, wg_ref, wu_ref, wd_ref, out_ref,
                 *rest[FLOW_SCRATCH:])


FLOW_SCRATCH = 21


def layer(sizes, r, k, v, d, b, gate, gain, res, w, ngain, ids, weights, wg, wu, wd):
    nz, ny, nx = sizes
    tokens, wide = r.shape
    part = wide // 2
    tp = ny * nx
    nstep = max(nz.bit_length() - 2, 0)
    ff = wg.shape[1]
    count = 2 * nz
    cap = 2 * tokens * ids.shape[1] // count
    rows = 2 * cap
    dma = pltpu.SemaphoreType.DMA
    vm = pl.BlockSpec(memory_space=pltpu.VMEM)
    hbm = pl.BlockSpec(memory_space=pl.ANY)
    square = (tokens, wide)
    flow_scratch = [
        pltpu.VMEM((2 * CHUNK, part), BF16),
        pltpu.VMEM((2 * CHUNK, part), BF16),
        pltpu.VMEM((nstep + 1, 2 * CHUNK, part), BF16),
        pltpu.VMEM((max(nstep, 1), 2 * CHUNK, part), BF16),
        pltpu.VMEM((2 * CHUNK, part), BF16),
        pltpu.VMEM((CHUNK, part), BF16),
        pltpu.VMEM((CHUNK, part), BF16),
        pltpu.VMEM((CHUNK, part), BF16),
        pltpu.VMEM((CHUNK, part), BF16),
        pltpu.VMEM((tp,) + square, BF16),
        pltpu.VMEM(square, F32),
        pltpu.VMEM((8, tokens), F32),
        pltpu.VMEM((tp - 1, 8, tokens), F32),
        dma((2,)),
        dma((2, max(nstep, 1))),
        dma((4,)),
        dma((2,)),
        dma((2 * (tp - 1),)),
        dma((2, tp)),
        dma((tp - 1,)),
        dma((tp - 1,)),
    ]
    expert_scratch = [
        pltpu.VMEM((count, cap, wide), BF16),
        pltpu.VMEM((count, cap, wide), BF16),
        pltpu.VMEM((nz, 2, rows, ff), BF16),
        pltpu.VMEM((nx, ny, rows, ff), BF16),
        pltpu.VMEM((ny, nx, rows, ff), BF16),
        pltpu.VMEM((ny - 1, rows, ff), BF16),
        pltpu.VMEM((nx - 1, rows, ff), BF16),
        pltpu.VMEM((ny - 1, rows, ff), BF16),
        pltpu.VMEM((nx - 1, rows, ff), BF16),
        pltpu.VMEM((tp, rows, ff), BF16),
        pltpu.VMEM((nz, 2, cap, wide), BF16),
        pltpu.VMEM((count, cap, wide), BF16),
        pltpu.VMEM((tokens, count * cap), BF16),
        pltpu.VMEM((tokens, count * cap), BF16),
        dma((count - 1,)),
        dma((count,)),
        dma((nz,)),
        dma((nx, ny)),
        dma((nz,)),
        dma((ny, nx)),
        dma((ny - 1,)),
        dma((ny - 1,)),
        dma((nx - 1,)),
        dma((nx - 1,)),
        dma((2 * (tp - 1),)),
        dma((2, tp)),
        dma((nz, 2)),
        dma((count,)),
    ]
    return pl.pallas_call(
        functools.partial(layer_body, nz, ny, nx),
        out_shape=jax.ShapeDtypeStruct(square, BF16),
        in_specs=[hbm] * 6 + [vm] + [hbm] * 2 + [vm] * 3 + [hbm] * 3,
        out_specs=vm,
        scratch_shapes=[pltpu.VMEM(square, BF16)] * 7
        + [
            pltpu.VMEM(w.shape, BF16),
            pltpu.VMEM(wg.shape, BF16),
            pltpu.VMEM(wu.shape, BF16),
            pltpu.VMEM(wd.shape, BF16),
            pltpu.VMEM(square, F32),
            pltpu.VMEM(square, F32),
            pltpu.VMEM((2 * CHUNK, wide), F32),
            pltpu.VMEM(square, BF16),
            pltpu.VMEM(square, BF16),
            dma((11,)),
        ]
        + flow_scratch
        + expert_scratch,
        compiler_params=pltpu.CompilerParams(
            collective_id=0, has_side_effects=True, vmem_limit_bytes=60 * 1024 * 1024
        ),
        name="layer",
    )(r, k, v, d, b, gate, gain, res, w, ngain, ids, weights, wg, wu, wd)


def local(
    receptance,
    key_vectors,
    value_vectors,
    decay_logits,
    rate_logits,
    gate_logits,
    group_gain,
    residual,
    mixer_out,
    norm_gain,
    expert_ids,
    route_weight,
    expert_gate,
    expert_up,
    expert_down,
):
    sizes = tuple(lax.axis_size(name) for name in ("z", "y", "x"))
    features = residual.shape[1]
    return layer(
        sizes,
        receptance,
        key_vectors,
        value_vectors,
        decay_logits,
        rate_logits,
        gate_logits,
        group_gain[None],
        residual,
        mixer_out.reshape(sizes[1] * sizes[2], -1, features),
        norm_gain[None],
        expert_ids,
        route_weight,
        expert_gate[0],
        expert_up[0],
        expert_down[0],
    )


def solution(mesh):
    torus = Mesh(mesh.devices.reshape(16, 2, 4, 4), ("z", "c", "y", "x"))
    return jax.shard_map(
        local,
        mesh=torus,
        in_specs=(
            P(SP, TP),
            P(SP, TP),
            P(SP, TP),
            P(SP, TP),
            P(SP, TP),
            P(SP, TP),
            P(TP),
            P(SP, TP),
            P(None, TP),
            P(TP),
            P(SP, None),
            P(SP, None),
            P(SP, TP, None),
            P(SP, TP, None),
            P(SP, None, TP),
        ),
        out_specs=P(SP, TP),
        check_vma=False,
    )
```

```python
import functools
import jax
import jax.numpy as jnp
from jax import lax
from jax.experimental import pallas as pl
from jax.experimental.pallas import tpu as pltpu
from jax.sharding import Mesh
from jax.sharding import PartitionSpec as P

SP = ("z", "c")
TP = ("y", "x")
F32 = jnp.float32
BF16 = jnp.bfloat16
CHUNK = 64


def iota2(shape, dim):
    return lax.broadcasted_iota(jnp.int32, shape, dim)


def halves(x):
    hi = x.astype(BF16)
    return hi, (x - hi.astype(F32)).astype(BF16)


def dot_dims(a, b, dims):
    return lax.dot_general(a, b, (dims, ((), ())), preferred_element_type=F32)


NN = ((1,), (0,))
NT = ((1,), (1,))
TN = ((0,), (0,))


def both_rows(x):
    hi, lo = halves(x)
    return jnp.concatenate([hi, lo], axis=0)


def left_split(a, b, dims=NN):
    rows = a.shape[0]
    full = dot_dims(both_rows(a), b, dims)
    return full[:rows] + full[rows:]


def two_split(a, b_hi, b_lo, dims=NN):
    rows = a.shape[0]
    hi, lo = halves(a)
    full = dot_dims(jnp.concatenate([hi, lo], axis=0), b_hi, dims)
    return full[:rows] + full[rows:] + dot_dims(hi, b_lo, dims)


def block_diag(x, mask):
    return jnp.concatenate([x] * (mask.shape[0] // x.shape[0]), axis=0) * mask


def block_dot(a, b, mask, dims=NN):
    b_hi, b_lo = halves(b)
    return two_split(a, block_diag(b_hi, mask), block_diag(b_lo, mask), dims)


def mix_body(r_ref, k_ref, v_ref, d_ref, b_ref, rd_ref, th_ref, ma_ref):
    tokens, width = r_ref.shape
    n = tokens // CHUNK
    row = iota2((width, width), 0)
    col = iota2((width, width), 1)
    same = (row // CHUNK) == (col // CHUNK)
    mask = same.astype(F32).astype(BF16)
    diag = row == col
    pos_t = iota2((CHUNK, width), 0)
    pos_s = iota2((CHUNK, width), 1) % CHUNK
    strict = pos_s < pos_t
    causal = pos_s <= pos_t
    eye_cat = (pos_s == pos_t).astype(F32)
    tri = (iota2((CHUNK, CHUNK), 1) <= iota2((CHUNK, CHUNK), 0)).astype(F32).astype(BF16)
    st = []
    for c in range(n):
        rows = pl.ds(c * CHUNK, CHUNK)
        recept = r_ref[rows, :].astype(F32)
        keyvec = k_ref[rows, :].astype(F32)
        val = v_ref[rows, :]
        logdec = (-0.6065306597126334) / (1.0 + jnp.exp(-d_ref[rows, :].astype(F32)))
        rate = 1.0 / (1.0 + jnp.exp(-b_ref[rows, :].astype(F32)))
        sums = left_split(keyvec * keyvec, mask)
        unit = keyvec * lax.rsqrt(1.0 + sums)
        corr = unit * rate
        ld_hi, ld_lo = halves(logdec)
        cum_in = dot_dims(tri, ld_hi, NN) + dot_dims(tri, ld_lo, NN)
        cum_ex = cum_in - logdec
        cum_end = cum_in[CHUNK - 1 : CHUNK, :]
        growth = jnp.exp(-cum_in)
        tail = jnp.exp(cum_end - cum_in)
        r_s = recept * jnp.exp(cum_in)
        u_s = unit * jnp.exp(cum_ex)
        st.append(dict(val=val, r_s=r_s, u_s=u_s, k_s=keyvec * growth, c_s=corr * growth,
                       c_tail=corr * tail, k_tail=keyvec * tail, keep=jnp.exp(cum_end)))
    for q in st:
        ur = jnp.concatenate([q["u_s"], q["r_s"]], axis=0)
        g_k = block_dot(ur, q["k_s"], mask, NT)
        g_c = block_dot(ur, q["c_s"], mask, NT)
        q["key_pull"] = jnp.where(strict, g_k[:CHUNK], 0.0)
        q["key_read"] = jnp.where(causal, g_k[CHUNK:], 0.0)
        q["low"] = jnp.where(strict, g_c[:CHUNK], 0.0)
        q["corr_read"] = jnp.where(causal, g_c[CHUNK:], 0.0)
        first = ((pos_t // 2) == (pos_s // 2)) & (pos_s < pos_t)
        q["x"] = eye_cat - jnp.where(first, q["low"], 0.0)
    size = 2
    while size < CHUNK:
        level = ((pos_t // (2 * size)) == (pos_s // (2 * size))) & ((pos_t // size) > (pos_s // size))
        for q in st:
            q["t"] = block_dot(q["x"], jnp.where(level, q["low"], 0.0), mask)
        for q in st:
            q["x"] = q["x"] - block_dot(q["t"], q["x"], mask)
        size *= 2
    for q in st:
        rl = left_split(jnp.concatenate([q["key_pull"], q["key_read"]], axis=0),
                        block_diag(q["val"], mask))
        q["right"], q["read"] = rl[:CHUNK], rl[CHUNK:]
    for q in st:
        q["pulled"] = block_dot(q["x"], q["right"], mask)
        q["reach"] = block_dot(q["x"], q["u_s"], mask)
    for q in st:
        q["read"] = q["read"] - block_dot(q["corr_read"], q["pulled"], mask)
        q["start"] = q["r_s"] - block_dot(q["corr_read"], q["reach"], mask)
        c_hi, c_lo = halves(q["c_tail"])
        k_hi, k_lo = halves(q["k_tail"])
        rh, rl_ = halves(q["reach"])
        full = (dot_dims(jnp.concatenate([rh, rl_, rh], axis=0),
                         jnp.concatenate([c_hi, c_hi, c_lo], axis=0), TN))
        q["map"] = jnp.where(same, jnp.where(diag, q["keep"], 0.0) - full, 0.0)
        ph, pl_ = halves(-q["pulled"])
        full = dot_dims(jnp.concatenate([q["val"], q["val"]], axis=0),
                        jnp.concatenate([k_hi, k_lo], axis=0), TN)
        full = full + dot_dims(jnp.concatenate([ph, pl_, ph], axis=0),
                               jnp.concatenate([c_hi, c_hi, c_lo], axis=0), TN)
        full = jnp.where(same, full, 0.0)
        q["add"] = sum(full[g * CHUNK : (g + 1) * CHUNK] for g in range(1, width // CHUNK)) + full[:CHUNK]
    ps = None
    for c, q in enumerate(st):
        rows = pl.ds(c * CHUNK, CHUNK)
        if c == 0:
            rd_ref[rows, :] = q["read"]
            th_ref[rows, :] = q["start"]
            m = q["map"]
            p = sum(m[g * CHUNK : (g + 1) * CHUNK] for g in range(1, width // CHUNK)) + m[:CHUNK]
            ps = jnp.concatenate([p, q["add"]], axis=0)
        else:
            th_ref[rows, :] = block_dot(q["start"], ps[:CHUNK], mask, NT)
            rd_ref[rows, :] = q["read"] + block_dot(q["start"], ps[CHUNK:], mask, NT)
            m_hi, m_lo = halves(q["map"])
            ps = two_split(ps, m_hi, m_lo)
            ps = jnp.concatenate([ps[:CHUNK], ps[CHUNK:] + q["add"]], axis=0)
    ma_ref[...] = ps


MESH = pl.DeviceIdType.MESH
EPS_GROUP = 0.00064
EPS_NORM = 1e-06


def ring_order(size):
    near = sorted(range(1, size), key=lambda k: (min(k, size - k), k))
    return near


def remote(src, dst, send, recv, **where):
    return pltpu.make_async_remote_copy(
        src_ref=src, dst_ref=dst, send_sem=send, recv_sem=recv, device_id=where, device_id_type=MESH
    )


def share_blocks(buf, send, recv, y, x, ny, nx, use):
    mine = y * nx + x
    half = buf.shape[1] // 2
    sent = []

    def view(slot, part):
        return buf.at[slot, pl.ds(part * half, half), :]

    def push(slot, part, **where):
        copy = remote(view(slot, part), view(slot, part), send.at[len(sent)], recv.at[part, slot], **where)
        copy.start()
        sent.append(copy)

    def arrived(slot, part):
        remote(view(slot, part), view(slot, part), send.at[0], recv.at[part, slot], x=x).wait_recv()

    xs, ys = ring_order(nx), ring_order(ny)
    for k in range(max(len(xs), len(ys))):
        if k < len(xs):
            push(mine, 0, x=lax.rem(x + xs[k], nx))
        if k < len(ys):
            push(mine, 1, y=lax.rem(y + ys[k], ny))
    for k in ys:
        push(mine, 0, y=lax.rem(y + k, ny))
    for k in xs:
        push(mine, 1, x=lax.rem(x + k, nx))
    use(mine, 0, 0, 0)
    use(mine, 1, 0, 0)
    for k in range(max(len(xs), len(ys))):
        if k < len(xs):
            slot = y * nx + lax.rem(x + nx - xs[k], nx)
            arrived(slot, 0)
            for j in ys:
                push(slot, 0, y=lax.rem(y + j, ny))
            use(slot, 0, 0, xs[k])
        if k < len(ys):
            slot = lax.rem(y + ny - ys[k], ny) * nx + x
            arrived(slot, 1)
            for j in xs:
                push(slot, 1, x=lax.rem(x + j, nx))
            use(slot, 1, ys[k], 0)
    for a in range(max(len(xs), len(ys))):
        for b in range(max(nx, ny)):
            if a < len(ys) and b < nx:
                slot = lax.rem(y + ny - ys[a], ny) * nx + lax.rem(x + nx - b, nx)
                arrived(slot, 0)
                use(slot, 0, ys[a], b)
            if a < len(xs) and b < ny:
                slot = lax.rem(y + ny - b, ny) * nx + lax.rem(x + nx - xs[a], nx)
                arrived(slot, 1)
                use(slot, 1, b, xs[a])
    return sent


def flow_body(nz, ny, nx, rd_ref, th_ref, ma_ref, gate_ref, gain_ref, res_ref, ngain_ref, w_ref,
              mid_ref, norm_ref, meanwhile,
              pair_out, pair_in, hop_out, hop_in, near_in, far_out, far_in, back_out, back_in,
              blocks, total, sq_out, sq_in,
              pair_s, hop_s, fin_s, back_s, ag_send, ag_recv, sq_send, sq_recv):
    z, c, y, x = (lax.axis_index(name) for name in ("z", "c", "y", "x"))
    steps = []
    d = 1
    while d < nz // 2:
        steps.append(d)
        d *= 2
    far = nz // 2 + 1
    xs, ys = ring_order(nx), ring_order(ny)
    plane = [(a, b) for a in range(ny) for b in range(nx) if (a, b) != (0, 0)]
    wide = ma_ref.shape[1]
    part = wide // 2
    ends = ma_ref[...]
    low, high = ends[:, :part], ends[:, part:]
    first = c == 0
    pair_out[...] = jnp.where(first, high, low).astype(BF16)
    swap = remote(pair_out, pair_in, pair_s.at[0], pair_s.at[1], c=1 - c)
    swap.start()
    mine = jnp.where(first, low, high)
    mask = ((iota2((part, part), 0) // CHUNK) == (iota2((part, part), 1) // CHUNK)).astype(F32).astype(BF16)
    with jax.named_scope("pair"):
        swap.wait()
    peer = pair_in[...].astype(F32)
    early = jnp.where(first, mine, peer)
    late = jnp.where(first, peer, mine)

    def compose(before, after):
        moved = block_dot(before, after[:CHUNK], mask)
        return jnp.concatenate([moved[:CHUNK], moved[CHUNK:] + after[CHUNK:]], axis=0)

    cur = compose(early, late)
    for i, d in enumerate(steps):
        hop_out[i] = cur.astype(BF16)
        hop = remote(hop_out.at[i], hop_in.at[i], hop_s.at[0, i], hop_s.at[1, i], z=lax.rem(z + d, nz))
        hop.start()
        if d == steps[-1]:
            meanwhile()
        with jax.named_scope(f"hop{d}"):
            hop.wait()
        joined = compose(hop_in[i].astype(F32), cur)
        cur = jnp.where(z >= d, joined, cur)
    last = len(steps)
    hop_out[last] = cur.astype(BF16)
    far_out[...] = cur[CHUNK:].astype(BF16)
    far_copy = remote(far_out, far_in, fin_s.at[0], fin_s.at[1], z=lax.rem(z + far, nz))
    far_copy.start()
    near_copy = remote(hop_out.at[last], near_in, fin_s.at[2], fin_s.at[3], z=lax.rem(z + 1, nz))
    near_copy.start()
    with jax.named_scope("near"):
        near_copy.wait()
    near = jnp.where(z >= 1, near_in[...].astype(F32), 0.0)
    with jax.named_scope("far"):
        far_copy.wait()
    far_add = jnp.where(z >= far, far_in[...].astype(F32), 0.0)
    start0 = block_dot(far_add, near[:CHUNK], mask) + near[CHUNK:]
    start1 = block_dot(start0, early[:CHUNK], mask) + early[CHUNK:]
    own = jnp.where(first, start0, start1)
    back_out[...] = jnp.where(first, start1, start0).astype(BF16)
    back = remote(back_out, back_in, back_s.at[0], back_s.at[1], c=1 - c)
    back.start()
    with jax.named_scope("back"):
        back.wait()
    other = back_in[...].astype(F32)
    incoming = jnp.concatenate([jnp.where(first, own, other), jnp.where(first, other, own)], axis=1)

    mask4 = ((iota2((wide, wide), 0) // CHUNK) == (iota2((wide, wide), 1) // CHUNK)).astype(F32).astype(BF16)
    read = rd_ref[...] + block_dot(th_ref[...], incoming, mask4, NT)
    centred = read - left_split(read, mask4) * (1.0 / CHUNK)
    spread = left_split(centred * centred, mask4) * (1.0 / CHUNK)
    gate = 1.0 / (1.0 + jnp.exp(-gate_ref[...].astype(F32)))
    mixed = centred * lax.rsqrt(spread + EPS_GROUP) * gain_ref[...] * gate
    tp = y * nx + x
    blocks[tp] = mixed.astype(BF16)
    total[...] = res_ref[...].astype(F32)
    half = blocks.shape[1] // 2

    def project(slot, part_no, *place):
        rows = pl.ds(part_no * half, half)
        total[rows, :] += jnp.dot(blocks[slot, rows, :], w_ref[slot], preferred_element_type=F32)

    with jax.named_scope("share"):
        sent = share_blocks(blocks, ag_send, ag_recv, y, x, ny, nx, project)
    midway = total[...].astype(BF16)
    mid_ref[...] = midway
    mid_f = midway.astype(F32)
    s_hi, s_lo = halves(mid_f * mid_f)
    ones = jnp.ones((8, wide), BF16)
    sums = dot_dims(ones, s_hi, NT) + dot_dims(ones, s_lo, NT)
    sq_out[...] = sums
    pieces = []
    for i, (a, b) in enumerate(plane):
        copy = remote(sq_out, sq_in.at[i], sq_send.at[i], sq_recv.at[i],
                      y=lax.rem(y + a, ny), x=lax.rem(x + b, nx))
        copy.start()
        pieces.append(copy)
    norm_ref[...] = (mid_f * ngain_ref[...]).astype(BF16)

    def inverse_rms():
        total_sq = sq_out[...]
        for i, copy in enumerate(pieces):
            copy.wait_recv()
            total_sq = total_sq + sq_in[i]
        return lax.rsqrt(total_sq * (1.0 / (wide * ny * nx)) + EPS_NORM)

    return inverse_rms, sent + pieces


def trade_weights(ny, nx, wg_ref, wu_ref, w_a, w_b, wt_s, wt_r):
    y, x = lax.axis_index("y"), lax.axis_index("x")
    ff = wg_ref.shape[1]
    copies = []
    for part, (name, at, n, dst) in enumerate((("x", x, nx, w_a), ("y", y, ny, w_b))):
        cut = ff // n
        for k in ring_order(n):
            to = lax.rem(at + k, n)
            cols = pl.ds(pl.multiple_of(to * cut, cut), cut)
            for which, src in enumerate((wg_ref, wu_ref)):
                copy = remote(src.at[:, cols], dst.at[at, which], wt_s.at[part, which, to],
                              wt_r.at[part, which, at], **{name: to})
                copy.start()
                copies.append(copy)
    for part, (at, n, dst) in enumerate(((x, nx, w_a), (y, ny, w_b))):
        cut = ff // n
        cols = pl.ds(pl.multiple_of(at * cut, cut), cut)
        dst[at, 0] = wg_ref[:, cols]
        dst[at, 1] = wu_ref[:, cols]

    def finish():
        for copy in copies:
            copy.wait_send()
        for part, (at, n, dst) in enumerate(((x, nx, w_a), (y, ny, w_b))):
            for k in ring_order(n):
                src = lax.rem(at + k, n)
                for which in (0, 1):
                    got = dst.at[src, which]
                    remote(got, got, wt_s.at[part, which, 0], wt_r.at[part, which, src], c=1 - lax.axis_index("c")).wait_recv()

    return finish


def prepare_routes(cap, slots, ids_ref, rw_ref, taken, turned, pick_hi, pick_lo):
    tokens = ids_ref.shape[0]
    ids = ids_ref[...]
    id0, id1 = ids[:, 0:1], ids[:, 1:2]
    lane = iota2((tokens, 128), 1)
    hit = jnp.where((lane == id0) | (lane == id1), 1.0, 0.0).astype(BF16)
    tri = jnp.where(iota2((tokens, tokens), 1) < iota2((tokens, tokens), 0), 1.0, 0.0).astype(BF16)
    earlier = dot_dims(tri, hit, NN)

    def slot_of(one):
        rank = jnp.sum(jnp.where(lane == one, earlier, 0.0), axis=1, keepdims=True)
        return one * cap + rank.astype(jnp.int32)

    slot0, slot1 = slot_of(id0), slot_of(id1)
    spot = iota2((tokens, slots), 1)
    hot0, hot1 = spot == slot0, spot == slot1
    take = jnp.where(hot0 | hot1, 1.0, 0.0).astype(BF16)
    rw = rw_ref[...]
    weight = jnp.where(hot0, rw[:, 0:1], 0.0) + jnp.where(hot1, rw[:, 1:2], 0.0)
    w_hi, w_lo = halves(weight)
    pick_hi[...] = w_hi
    pick_lo[...] = w_lo
    taken[...] = take
    eye = (iota2((tokens, tokens), 0) == iota2((tokens, tokens), 1)).astype(F32).astype(BF16)
    turned[...] = dot_dims(take, eye, TN).astype(BF16)


def experts_body(nz, ny, nx, inverse_rms, norm_ref, mid_ref, w_a, w_b, wd_ref, out_ref,
                 taken, turned, pick_hi, pick_lo, going, came, rows_a, rows_b, half_a, half_b, got_a, got_b, own_a, own_b,
                 hid, res, back, scale_out, scale_in, scale_col,
                 go_s, go_r, x_s, x_r, y_s, y_r, a_s, a_r, b_s, b_r, ag_send, ag_recv, re_s, re_r, sc_s, sc_r):
    z, c, y, x = (lax.axis_index(name) for name in ("z", "c", "y", "x"))
    me = 2 * z + c
    tp = y * nx + x
    count, cap, wide = going.shape
    slots = count * cap
    xs, ys = ring_order(nx), ring_order(ny)

    going[...] = dot_dims(turned[...], norm_ref[...], NN).astype(BF16).reshape(going.shape)

    nh = nz // 2
    offs = [0] + [o for d in range(1, nh) for o in (d, nz - d)] + [nh]
    sent = []

    def dispatch(zt, ct):
        copy = remote(going.at[2 * zt + ct], came.at[me], go_s.at[len(sent)], go_r.at[me], z=zt, c=ct)
        copy.start()
        sent.append(copy)

    def dispatch_to(ct):
        for o in offs[1:]:
            dispatch(lax.rem(z + nz - o, nz), ct)

    came[me] = going[me]
    dispatch(z, 1 - c)
    dispatch_to(0)
    group = 128 // cap
    line = jnp.where(c == 0, lax.div(z, nx), lax.rem(z, nx))
    speaks = line == jnp.where(c == 0, y, x)
    place = jnp.where(c == 0, lax.rem(z, nx), lax.div(z, nx))

    def scale_to(e):
        return remote(scale_out.at[lax.div(e, group)], scale_in.at[c, place], sc_s.at[e], sc_r.at[c, place],
                      z=lax.div(e, 2), c=lax.rem(e, 2))

    def tell_scale():
        inv = inverse_rms()
        i_hi, i_rest = halves(inv)
        i_mid, i_lo = halves(inv - i_hi.astype(F32))
        spread = (dot_dims(i_hi, taken[...], NN) + dot_dims(i_mid, taken[...], NN)
                  + dot_dims(i_lo, taken[...], NN))
        for g in range(slots // 128):
            scale_out[g] = spread[:, g * 128 : (g + 1) * 128]

        @pl.when(speaks)
        def _():
            def tell(e, carry):
                @pl.when(e != me)
                def _():
                    scale_to(e).start()

                return carry

            lax.fori_loop(0, count, tell, 0)
            scale_in[c, place] = scale_out[lax.div(me, group)]

    tell_scale()
    dispatch_to(1)

    def take_in(src):
        @pl.when(src != me)
        def _():
            remote(came.at[src], came.at[src], go_s.at[0], go_r.at[src], c=1 - c).wait_recv()

    def onward(t):
        copies = [remote(came.at[2 * t], rows_a.at[x, t], x_s.at[k - 1, t], x_r.at[x, t], x=lax.rem(x + k, nx))
                  for k in xs]
        copies += [remote(came.at[2 * t + 1], rows_b.at[y, t], y_s.at[k - 1, t], y_r.at[y, t], y=lax.rem(y + k, ny))
                   for k in ys]
        return copies

    def receive(t):
        take_in(2 * t)
        take_in(2 * t + 1)
        for copy in onward(t):
            copy.start()

    def settle_a(t):
        ty, tx = lax.div(t, nx), lax.rem(t, nx)
        return remote(half_a.at[t], got_a.at[y, tx], a_s.at[t], a_r.at[y, tx], y=ty)

    def settle_b(t):
        ty, tx = lax.div(t, nx), lax.rem(t, nx)
        return remote(half_b.at[t], got_b.at[x, ty], b_s.at[t], b_r.at[x, ty], x=tx)

    def partials(t):
        ty, tx = lax.div(t, nx), lax.rem(t, nx)
        for part, (places, at, n, rows, recv, w, out, own, mine, spot_own, settle) in enumerate((
            (xs, x, nx, rows_a, x_r, w_a, half_a, own_a, ty == y, tx, settle_a),
            (ys, y, ny, rows_b, y_r, w_b, half_b, own_b, tx == x, ty, settle_b),
        )):
            first = came[2 * t + part]
            gate = jnp.dot(first, w[at, 0], preferred_element_type=F32)
            up = jnp.dot(first, w[at, 1], preferred_element_type=F32)
            for k in places:
                src = lax.rem(at + n - k, n)
                got = rows.at[src, t]
                remote(got, got, go_s.at[0], recv.at[src, t], c=1 - c).wait_recv()
                value = rows[src, t]
                gate = gate + jnp.dot(value, w[src, 0], preferred_element_type=F32)
                up = up + jnp.dot(value, w[src, 1], preferred_element_type=F32)
            cut = gate.shape[1]

            @pl.when(mine)
            def _(own=own, spot_own=spot_own, gate=gate, up=up, cut=cut):
                own[spot_own, :, :cut] = gate
                own[spot_own, :, cut:] = up

            @pl.when(jnp.logical_not(mine))
            def _(out=out, settle=settle, gate=gate, up=up, cut=cut):
                out[t, :, :cut] = gate.astype(BF16)
                out[t, :, cut:] = up.astype(BF16)
                settle(t).start()

    def block_at(i):
        d = lax.div(i + 1, 2)
        off = jnp.where(lax.rem(i, 2) == 1, d, lax.rem(nz - d, nz))
        return lax.rem(z + off, nz)

    def step(j, carry):
        @pl.when(j < nz)
        def _():
            receive(block_at(j))

        @pl.when(j >= LAG)
        def _():
            partials(block_at(j - LAG))

        return carry

    with jax.named_scope("pipeline"):
        lax.fori_loop(0, nz + LAG, step, 0)

    eighth = jnp.full((8, 128), 0.125, BF16)
    with jax.named_scope("activate"):
        for part, (places, at, n, m, got, recv, own) in enumerate((
            (ys, y, ny, nx, got_a, a_r, own_a),
            (xs, x, nx, ny, got_b, b_r, own_b),
        )):
            for i in range(m):
                from_z = y * nx + i if part == 0 else i * nx + x

                @pl.when(jnp.logical_not(jnp.logical_and(from_z == z, c == part)))
                def _(part=part, i=i):
                    ref = scale_in.at[part, i]
                    remote(ref, ref, sc_s.at[0], sc_r.at[part, i], c=1 - c).wait_recv()

                s_hi, s_rest = halves(scale_in[part, i])
                s_mid, s_lo = halves(scale_in[part, i] - s_hi.astype(F32))
                scale_col[...] = dot_dims(s_hi, eighth, TN) + dot_dims(s_mid, eighth, TN) + dot_dims(s_lo, eighth, TN)
                factor = scale_col[pl.ds(pl.multiple_of(lax.rem(me, group) * cap, cap), cap), :]
                total = own[i]
                cut = total.shape[1] // 2
                for k in places:
                    src = lax.rem(at + n - k, n)
                    ref = got.at[src, i]
                    remote(ref, ref, go_s.at[0], recv.at[src, i], c=1 - c).wait_recv()
                    total = total + got[src, i].astype(F32)
                total = total * jnp.concatenate([factor] * (2 * cut // 128), axis=1)
                gate, up = total[:, :cut], total[:, cut:]
                first_row = part * m * cap + i * cap
                hid[tp, first_row : first_row + cap, :] = (gate / (1.0 + jnp.exp(-gate)) * up).astype(BF16)

    def give_back(t, part):
        return remote(res.at[t, part], back.at[me], re_s.at[t, part], re_r.at[me], z=t, c=part)

    seen = {}
    half_rows = hid.shape[1] // 2

    def down(slot, part, dy, dx):
        key = (part, dy if part == 0 else dx)
        seen[key] = seen.get(key, 0) + 1
        n = nx if part == 0 else ny
        if seen[key] < n:
            return
        ry, rx = lax.rem(y + ny - dy, ny), lax.rem(x + nx - dx, nx)
        value = None
        for k in range(n):
            src = ry * nx + k if part == 0 else k * nx + rx
            term = jnp.dot(hid[src, part * half_rows : (part + 1) * half_rows, :], wd_ref[k], preferred_element_type=F32)
            value = term if value is None else value + term
        value = value.astype(BF16)
        for i in range(n):
            t = ry * nx + i if part == 0 else i * nx + rx
            piece = value[i * cap : (i + 1) * cap]
            res[t, part] = piece
            here = jnp.logical_and(t == z, c == part)

            @pl.when(here)
            def _(piece=piece):
                back[me] = piece

            @pl.when(jnp.logical_not(here))
            def _(t=t):
                give_back(t, part).start()

    with jax.named_scope("down"):
        shared = share_blocks(hid, ag_send, ag_recv, y, x, ny, nx, down)

    def collect(src, carry):
        @pl.when(src != me)
        def _():
            remote(back.at[src], back.at[src], re_s.at[0, 0], re_r.at[src], c=1 - c).wait_recv()

        return carry

    with jax.named_scope("collect"):
        lax.fori_loop(0, count, collect, 0)
    rows = back[...].reshape(slots, wide)
    routed = dot_dims(pick_hi[...], rows, NN) + dot_dims(pick_lo[...], rows, NN)
    out_ref[...] = (mid_ref[...].astype(F32) + routed).astype(BF16)

    for copy in sent + shared:
        copy.wait_send()

    def drain(t, carry):
        for copy in onward(t):
            copy.wait_send()

        @pl.when(lax.div(t, nx) != y)
        def _():
            settle_a(t).wait_send()

        @pl.when(lax.rem(t, nx) != x)
        def _():
            settle_b(t).wait_send()

        for part in (0, 1):
            @pl.when(jnp.logical_not(jnp.logical_and(t == z, c == part)))
            def _(part=part):
                give_back(t, part).wait_send()

            e = 2 * t + part

            @pl.when(jnp.logical_and(speaks, e != me))
            def _(e=e):
                scale_to(e).wait_send()

        return carry

    with jax.named_scope("drain"):
        lax.fori_loop(0, nz, drain, 0)


LAG = 6


def layer_body(nz, ny, nx, r_hbm, k_hbm, v_hbm, d_hbm, b_hbm, gate_hbm, gain_ref, res_hbm, w_hbm, ngain_ref,
               ids_ref, rw_ref, wg_hbm, wu_hbm, wd_hbm, out_ref,
               r_ref, k_ref, v_ref, d_ref, b_ref, gate_ref, res_ref, w_ref, wg_ref, wu_ref, wd_ref,
               rd_ref, th_ref, ma_ref, mid_ref, norm_ref, load_s, *rest):
    z, c, y, x = (lax.axis_index(name) for name in ("z", "c", "y", "x"))
    loads = [
        pltpu.make_async_copy(src, dst, load_s.at[i])
        for i, (src, dst) in enumerate((
            (d_hbm, d_ref), (k_hbm, k_ref), (b_hbm, b_ref), (r_hbm, r_ref), (v_hbm, v_ref),
            (gate_hbm, gate_ref), (res_hbm, res_ref), (w_hbm, w_ref),
            (wg_hbm, wg_ref), (wu_hbm, wu_ref), (wd_hbm, wd_ref),
        ))
    ]
    for copy in loads:
        copy.start()
    barrier = pltpu.get_barrier_semaphore()
    plane = [(a, b) for a in range(ny) for b in range(nx) if (a, b) != (0, 0)]
    who = [dict(c=1 - c)]
    who += [dict(z=lax.rem(z + o, nz), c=1 - c if f else c) for o in ring_order(nz) for f in (0, 1)]
    who += [dict(y=lax.rem(y + a, ny), x=lax.rem(x + b, nx)) for a, b in plane]
    for where in who:
        pl.semaphore_signal(barrier, inc=1, device_id=where, device_id_type=MESH)
    for copy in loads[:5]:
        copy.wait()
    with jax.named_scope("mix"):
        mix_body(r_ref, k_ref, v_ref, d_ref, b_ref, rd_ref, th_ref, ma_ref)
    with jax.named_scope("meet"):
        pl.semaphore_wait(barrier, len(who))
        for copy in loads[5:]:
            copy.wait()
    routes = rest[FLOW_SCRATCH + 4 : FLOW_SCRATCH + 8]
    slots, cap = routes[1].shape[0], routes[1].shape[0] // (2 * nz)
    meanwhile = functools.partial(prepare_routes, cap, slots, ids_ref, rw_ref, *routes)
    finish_trade = trade_weights(ny, nx, wg_ref, wu_ref, *rest[FLOW_SCRATCH : FLOW_SCRATCH + 4])
    inverse_rms, sent = flow_body(nz, ny, nx, rd_ref, th_ref, ma_ref, gate_ref, gain_ref, res_ref, ngain_ref, w_ref,
              mid_ref, norm_ref, meanwhile, *rest[:FLOW_SCRATCH])
    finish_trade()
    w_a, w_b = rest[FLOW_SCRATCH], rest[FLOW_SCRATCH + 1]
    experts_body(nz, ny, nx, inverse_rms, norm_ref, mid_ref, w_a, w_b, wd_ref, out_ref,
                 *rest[FLOW_SCRATCH + 4 :])
    for copy in sent:
        copy.wait_send()


FLOW_SCRATCH = 21


def layer(sizes, r, k, v, d, b, gate, gain, res, w, ngain, ids, weights, wg, wu, wd):
    nz, ny, nx = sizes
    tokens, wide = r.shape
    part = wide // 2
    tp = ny * nx
    nstep = max(nz.bit_length() - 2, 0)
    ff = wg.shape[1]
    count = 2 * nz
    cap = 2 * tokens * ids.shape[1] // count
    rows = 2 * cap
    wd = wd.reshape(nx, ff // nx, wide)
    dma = pltpu.SemaphoreType.DMA
    vm = pl.BlockSpec(memory_space=pltpu.VMEM)
    hbm = pl.BlockSpec(memory_space=pl.ANY)
    square = (tokens, wide)
    flow_scratch = [
        pltpu.VMEM((2 * CHUNK, part), BF16),
        pltpu.VMEM((2 * CHUNK, part), BF16),
        pltpu.VMEM((nstep + 1, 2 * CHUNK, part), BF16),
        pltpu.VMEM((max(nstep, 1), 2 * CHUNK, part), BF16),
        pltpu.VMEM((2 * CHUNK, part), BF16),
        pltpu.VMEM((CHUNK, part), BF16),
        pltpu.VMEM((CHUNK, part), BF16),
        pltpu.VMEM((CHUNK, part), BF16),
        pltpu.VMEM((CHUNK, part), BF16),
        pltpu.VMEM((tp,) + square, BF16),
        pltpu.VMEM(square, F32),
        pltpu.VMEM((8, tokens), F32),
        pltpu.VMEM((tp - 1, 8, tokens), F32),
        dma((2,)),
        dma((2, max(nstep, 1))),
        dma((4,)),
        dma((2,)),
        dma((2 * (tp - 1),)),
        dma((2, tp)),
        dma((tp - 1,)),
        dma((tp - 1,)),
    ]
    cut = ff // nx
    trade_scratch = [
        pltpu.VMEM((nx, 2, wide, cut), BF16),
        pltpu.VMEM((ny, 2, wide, cut), BF16),
        dma((2, 2, nx)),
        dma((2, 2, nx)),
    ]
    expert_scratch = [
        pltpu.VMEM((tokens, count * cap), BF16),
        pltpu.VMEM((count * cap, tokens), BF16),
        pltpu.VMEM((tokens, count * cap), BF16),
        pltpu.VMEM((tokens, count * cap), BF16),
        pltpu.VMEM((count, cap, wide), BF16),
        pltpu.VMEM((count, cap, wide), BF16),
        pltpu.VMEM((nx, nz, cap, wide), BF16),
        pltpu.VMEM((ny, nz, cap, wide), BF16),
        pltpu.VMEM((nz, cap, 2 * cut), BF16),
        pltpu.VMEM((nz, cap, 2 * cut), BF16),
        pltpu.VMEM((ny, nx, cap, 2 * cut), BF16),
        pltpu.VMEM((nx, ny, cap, 2 * cut), BF16),
        pltpu.VMEM((nx, cap, 2 * cut), F32),
        pltpu.VMEM((ny, cap, 2 * cut), F32),
        pltpu.VMEM((tp, 2 * nx * cap, cut), BF16),
        pltpu.VMEM((nz, 2, cap, wide), BF16),
        pltpu.VMEM((count, cap, wide), BF16),
        pltpu.VMEM((count * cap // 128, 8, 128), F32),
        pltpu.VMEM((2, nx, 8, 128), F32),
        pltpu.VMEM((128, 128), F32),
        dma((count - 1,)),
        dma((count,)),
        dma((nx - 1, nz)),
        dma((nx, nz)),
        dma((ny - 1, nz)),
        dma((ny, nz)),
        dma((nz,)),
        dma((ny, nx)),
        dma((nz,)),
        dma((nx, ny)),
        dma((2 * (tp - 1),)),
        dma((2, tp)),
        dma((nz, 2)),
        dma((count,)),
        dma((count,)),
        dma((2, nx)),
    ]
    return pl.pallas_call(
        functools.partial(layer_body, nz, ny, nx),
        out_shape=jax.ShapeDtypeStruct(square, BF16),
        in_specs=[hbm] * 6 + [vm] + [hbm] * 2 + [vm] * 3 + [hbm] * 3,
        out_specs=vm,
        scratch_shapes=[pltpu.VMEM(square, BF16)] * 7
        + [
            pltpu.VMEM(w.shape, BF16),
            pltpu.VMEM(wg.shape, BF16),
            pltpu.VMEM(wu.shape, BF16),
            pltpu.VMEM(wd.shape, BF16),
            pltpu.VMEM(square, F32),
            pltpu.VMEM(square, F32),
            pltpu.VMEM((2 * CHUNK, wide), F32),
            pltpu.VMEM(square, BF16),
            pltpu.VMEM(square, BF16),
            dma((11,)),
        ]
        + flow_scratch
        + trade_scratch
        + expert_scratch,
        compiler_params=pltpu.CompilerParams(
            collective_id=0, has_side_effects=True, vmem_limit_bytes=60 * 1024 * 1024
        ),
        name="layer",
    )(r, k, v, d, b, gate, gain, res, w, ngain, ids, weights, wg, wu, wd)


def local(
    receptance,
    key_vectors,
    value_vectors,
    decay_logits,
    rate_logits,
    gate_logits,
    group_gain,
    residual,
    mixer_out,
    norm_gain,
    expert_ids,
    route_weight,
    expert_gate,
    expert_up,
    expert_down,
):
    sizes = tuple(lax.axis_size(name) for name in ("z", "y", "x"))
    features = residual.shape[1]
    return layer(
        sizes,
        receptance,
        key_vectors,
        value_vectors,
        decay_logits,
        rate_logits,
        gate_logits,
        group_gain[None],
        residual,
        mixer_out.reshape(sizes[1] * sizes[2], -1, features),
        norm_gain[None],
        expert_ids,
        route_weight,
        expert_gate[0],
        expert_up[0],
        expert_down[0],
    )


def solution(mesh):
    torus = Mesh(mesh.devices.reshape(16, 2, 4, 4), ("z", "c", "y", "x"))
    return jax.shard_map(
        local,
        mesh=torus,
        in_specs=(
            P(SP, TP),
            P(SP, TP),
            P(SP, TP),
            P(SP, TP),
            P(SP, TP),
            P(SP, TP),
            P(TP),
            P(SP, TP),
            P(None, TP),
            P(TP),
            P(SP, None),
            P(SP, None),
            P(SP, TP, None),
            P(SP, TP, None),
            P(SP, None, TP),
        ),
        out_specs=P(SP, TP),
        check_vma=False,
    )
```

```python
import functools
import jax
import jax.numpy as jnp
from jax import lax
from jax.experimental import pallas as pl
from jax.experimental.pallas import tpu as pltpu
from jax.sharding import Mesh
from jax.sharding import PartitionSpec as P

SP = ("z", "c")
TP = ("y", "x")
F32 = jnp.float32
BF16 = jnp.bfloat16
CHUNK = 64


def iota2(shape, dim):
    return lax.broadcasted_iota(jnp.int32, shape, dim)


def halves(x):
    hi = x.astype(BF16)
    return hi, (x - hi.astype(F32)).astype(BF16)


def dot_dims(a, b, dims):
    return lax.dot_general(a, b, (dims, ((), ())), preferred_element_type=F32)


NN = ((1,), (0,))
NT = ((1,), (1,))
TN = ((0,), (0,))


def both_rows(x):
    hi, lo = halves(x)
    return jnp.concatenate([hi, lo], axis=0)


def left_split(a, b, dims=NN):
    rows = a.shape[0]
    full = dot_dims(both_rows(a), b, dims)
    return full[:rows] + full[rows:]


def two_split(a, b_hi, b_lo, dims=NN):
    rows = a.shape[0]
    hi, lo = halves(a)
    full = dot_dims(jnp.concatenate([hi, lo], axis=0), b_hi, dims)
    return full[:rows] + full[rows:] + dot_dims(hi, b_lo, dims)


def block_diag(x, mask):
    return jnp.concatenate([x] * (mask.shape[0] // x.shape[0]), axis=0) * mask


def block_dot(a, b, mask, dims=NN):
    b_hi, b_lo = halves(b)
    return two_split(a, block_diag(b_hi, mask), block_diag(b_lo, mask), dims)


def mix_body(r_ref, k_ref, v_ref, d_ref, b_ref, rd_ref, th_ref, ma_ref):
    tokens, width = r_ref.shape
    n = tokens // CHUNK
    row = iota2((width, width), 0)
    col = iota2((width, width), 1)
    same = (row // CHUNK) == (col // CHUNK)
    mask = same.astype(F32).astype(BF16)
    diag = row == col
    pos_t = iota2((CHUNK, width), 0)
    pos_s = iota2((CHUNK, width), 1) % CHUNK
    strict = pos_s < pos_t
    causal = pos_s <= pos_t
    eye_cat = (pos_s == pos_t).astype(F32)
    tri = (iota2((CHUNK, CHUNK), 1) <= iota2((CHUNK, CHUNK), 0)).astype(F32).astype(BF16)
    st = []
    for c in range(n):
        rows = pl.ds(c * CHUNK, CHUNK)
        recept = r_ref[rows, :].astype(F32)
        keyvec = k_ref[rows, :].astype(F32)
        val = v_ref[rows, :]
        logdec = (-0.6065306597126334) / (1.0 + jnp.exp(-d_ref[rows, :].astype(F32)))
        rate = 1.0 / (1.0 + jnp.exp(-b_ref[rows, :].astype(F32)))
        sums = left_split(keyvec * keyvec, mask)
        unit = keyvec * lax.rsqrt(1.0 + sums)
        corr = unit * rate
        ld_hi, ld_lo = halves(logdec)
        cum_in = dot_dims(tri, ld_hi, NN) + dot_dims(tri, ld_lo, NN)
        cum_ex = cum_in - logdec
        cum_end = cum_in[CHUNK - 1 : CHUNK, :]
        growth = jnp.exp(-cum_in)
        tail = jnp.exp(cum_end - cum_in)
        r_s = recept * jnp.exp(cum_in)
        u_s = unit * jnp.exp(cum_ex)
        st.append(dict(val=val, r_s=r_s, u_s=u_s, k_s=keyvec * growth, c_s=corr * growth,
                       c_tail=corr * tail, k_tail=keyvec * tail, keep=jnp.exp(cum_end)))
    for q in st:
        ur = jnp.concatenate([q["u_s"], q["r_s"]], axis=0)
        g_k = block_dot(ur, q["k_s"], mask, NT)
        g_c = block_dot(ur, q["c_s"], mask, NT)
        q["key_pull"] = jnp.where(strict, g_k[:CHUNK], 0.0)
        q["key_read"] = jnp.where(causal, g_k[CHUNK:], 0.0)
        q["low"] = jnp.where(strict, g_c[:CHUNK], 0.0)
        q["corr_read"] = jnp.where(causal, g_c[CHUNK:], 0.0)
        first = ((pos_t // 2) == (pos_s // 2)) & (pos_s < pos_t)
        q["x"] = eye_cat - jnp.where(first, q["low"], 0.0)
    size = 2
    while size < CHUNK:
        level = ((pos_t // (2 * size)) == (pos_s // (2 * size))) & ((pos_t // size) > (pos_s // size))
        for q in st:
            q["t"] = block_dot(q["x"], jnp.where(level, q["low"], 0.0), mask)
        for q in st:
            q["x"] = q["x"] - block_dot(q["t"], q["x"], mask)
        size *= 2
    for q in st:
        rl = left_split(jnp.concatenate([q["key_pull"], q["key_read"]], axis=0),
                        block_diag(q["val"], mask))
        q["right"], q["read"] = rl[:CHUNK], rl[CHUNK:]
    for q in st:
        q["pulled"] = block_dot(q["x"], q["right"], mask)
        q["reach"] = block_dot(q["x"], q["u_s"], mask)
    for q in st:
        q["read"] = q["read"] - block_dot(q["corr_read"], q["pulled"], mask)
        q["start"] = q["r_s"] - block_dot(q["corr_read"], q["reach"], mask)
        c_hi, c_lo = halves(q["c_tail"])
        k_hi, k_lo = halves(q["k_tail"])
        rh, rl_ = halves(q["reach"])
        full = (dot_dims(jnp.concatenate([rh, rl_, rh], axis=0),
                         jnp.concatenate([c_hi, c_hi, c_lo], axis=0), TN))
        q["map"] = jnp.where(same, jnp.where(diag, q["keep"], 0.0) - full, 0.0)
        ph, pl_ = halves(-q["pulled"])
        full = dot_dims(jnp.concatenate([q["val"], q["val"]], axis=0),
                        jnp.concatenate([k_hi, k_lo], axis=0), TN)
        full = full + dot_dims(jnp.concatenate([ph, pl_, ph], axis=0),
                               jnp.concatenate([c_hi, c_hi, c_lo], axis=0), TN)
        full = jnp.where(same, full, 0.0)
        q["add"] = sum(full[g * CHUNK : (g + 1) * CHUNK] for g in range(1, width // CHUNK)) + full[:CHUNK]
    ps = None
    for c, q in enumerate(st):
        rows = pl.ds(c * CHUNK, CHUNK)
        if c == 0:
            rd_ref[rows, :] = q["read"]
            th_ref[rows, :] = q["start"]
            m = q["map"]
            p = sum(m[g * CHUNK : (g + 1) * CHUNK] for g in range(1, width // CHUNK)) + m[:CHUNK]
            ps = jnp.concatenate([p, q["add"]], axis=0)
        else:
            th_ref[rows, :] = block_dot(q["start"], ps[:CHUNK], mask, NT)
            rd_ref[rows, :] = q["read"] + block_dot(q["start"], ps[CHUNK:], mask, NT)
            m_hi, m_lo = halves(q["map"])
            ps = two_split(ps, m_hi, m_lo)
            ps = jnp.concatenate([ps[:CHUNK], ps[CHUNK:] + q["add"]], axis=0)
    ma_ref[...] = ps


MESH = pl.DeviceIdType.MESH
EPS_GROUP = 0.00064
EPS_NORM = 1e-06


def ring_order(size):
    near = sorted(range(1, size), key=lambda k: (min(k, size - k), k))
    return near


def remote(src, dst, send, recv, **where):
    return pltpu.make_async_remote_copy(
        src_ref=src, dst_ref=dst, send_sem=send, recv_sem=recv, device_id=where, device_id_type=MESH
    )


def share_blocks(buf, send, recv, y, x, ny, nx, use):
    mine = y * nx + x
    half = buf.shape[1] // 2
    sent = []

    def view(slot, part):
        return buf.at[slot, pl.ds(part * half, half), :]

    def push(slot, part, **where):
        copy = remote(view(slot, part), view(slot, part), send.at[len(sent)], recv.at[part, slot], **where)
        copy.start()
        sent.append(copy)

    def arrived(slot, part):
        remote(view(slot, part), view(slot, part), send.at[0], recv.at[part, slot], x=x).wait_recv()

    xs, ys = ring_order(nx), ring_order(ny)
    for k in range(max(len(xs), len(ys))):
        if k < len(xs):
            push(mine, 0, x=lax.rem(x + xs[k], nx))
        if k < len(ys):
            push(mine, 1, y=lax.rem(y + ys[k], ny))
    for k in ys:
        push(mine, 0, y=lax.rem(y + k, ny))
    for k in xs:
        push(mine, 1, x=lax.rem(x + k, nx))
    use(mine, 0, 0, 0)
    use(mine, 1, 0, 0)
    for k in range(max(len(xs), len(ys))):
        if k < len(xs):
            slot = y * nx + lax.rem(x + nx - xs[k], nx)
            arrived(slot, 0)
            for j in ys:
                push(slot, 0, y=lax.rem(y + j, ny))
            use(slot, 0, 0, xs[k])
        if k < len(ys):
            slot = lax.rem(y + ny - ys[k], ny) * nx + x
            arrived(slot, 1)
            for j in xs:
                push(slot, 1, x=lax.rem(x + j, nx))
            use(slot, 1, ys[k], 0)
    for a in range(max(len(xs), len(ys))):
        for b in range(max(nx, ny)):
            if a < len(ys) and b < nx:
                slot = lax.rem(y + ny - ys[a], ny) * nx + lax.rem(x + nx - b, nx)
                arrived(slot, 0)
                use(slot, 0, ys[a], b)
            if a < len(xs) and b < ny:
                slot = lax.rem(y + ny - b, ny) * nx + lax.rem(x + nx - xs[a], nx)
                arrived(slot, 1)
                use(slot, 1, b, xs[a])
    return sent


def flow_body(nz, ny, nx, rd_ref, th_ref, ma_ref, gate_ref, gain_ref, res_ref, ngain_ref, w_ref,
              mid_ref, norm_ref, meanwhile,
              pair_out, pair_in, hop_out, hop_in, near_in, far_out, far_in, back_out, back_in,
              blocks, total, sq_out, sq_in,
              pair_s, hop_s, fin_s, back_s, ag_send, ag_recv, sq_send, sq_recv):
    z, c, y, x = (lax.axis_index(name) for name in ("z", "c", "y", "x"))
    steps = []
    d = 1
    while d < nz // 2:
        steps.append(d)
        d *= 2
    far = nz // 2 + 1
    xs, ys = ring_order(nx), ring_order(ny)
    plane = [(a, b) for a in range(ny) for b in range(nx) if (a, b) != (0, 0)]
    wide = ma_ref.shape[1]
    part = wide // 2
    ends = ma_ref[...]
    low, high = ends[:, :part], ends[:, part:]
    first = c == 0
    pair_out[...] = jnp.where(first, high, low).astype(BF16)
    swap = remote(pair_out, pair_in, pair_s.at[0], pair_s.at[1], c=1 - c)
    swap.start()
    mine = jnp.where(first, low, high)
    mask = ((iota2((part, part), 0) // CHUNK) == (iota2((part, part), 1) // CHUNK)).astype(F32).astype(BF16)
    with jax.named_scope("pair"):
        swap.wait()
    peer = pair_in[...].astype(F32)
    early = jnp.where(first, mine, peer)
    late = jnp.where(first, peer, mine)

    def compose(before, after):
        moved = block_dot(before, after[:CHUNK], mask)
        return jnp.concatenate([moved[:CHUNK], moved[CHUNK:] + after[CHUNK:]], axis=0)

    cur = compose(early, late)
    for i, d in enumerate(steps):
        hop_out[i] = cur.astype(BF16)
        hop = remote(hop_out.at[i], hop_in.at[i], hop_s.at[0, i], hop_s.at[1, i], z=lax.rem(z + d, nz))
        hop.start()
        if d == steps[-1]:
            meanwhile()
        with jax.named_scope(f"hop{d}"):
            hop.wait()
        joined = compose(hop_in[i].astype(F32), cur)
        cur = jnp.where(z >= d, joined, cur)
    last = len(steps)
    hop_out[last] = cur.astype(BF16)
    far_out[...] = cur[CHUNK:].astype(BF16)
    far_copy = remote(far_out, far_in, fin_s.at[0], fin_s.at[1], z=lax.rem(z + far, nz))
    far_copy.start()
    near_copy = remote(hop_out.at[last], near_in, fin_s.at[2], fin_s.at[3], z=lax.rem(z + 1, nz))
    near_copy.start()
    with jax.named_scope("near"):
        near_copy.wait()
    near = jnp.where(z >= 1, near_in[...].astype(F32), 0.0)
    with jax.named_scope("far"):
        far_copy.wait()
    far_add = jnp.where(z >= far, far_in[...].astype(F32), 0.0)
    start0 = block_dot(far_add, near[:CHUNK], mask) + near[CHUNK:]
    start1 = block_dot(start0, early[:CHUNK], mask) + early[CHUNK:]
    own = jnp.where(first, start0, start1)
    back_out[...] = jnp.where(first, start1, start0).astype(BF16)
    back = remote(back_out, back_in, back_s.at[0], back_s.at[1], c=1 - c)
    back.start()
    with jax.named_scope("back"):
        back.wait()
    other = back_in[...].astype(F32)
    incoming = jnp.concatenate([jnp.where(first, own, other), jnp.where(first, other, own)], axis=1)

    mask4 = ((iota2((wide, wide), 0) // CHUNK) == (iota2((wide, wide), 1) // CHUNK)).astype(F32).astype(BF16)
    read = rd_ref[...] + block_dot(th_ref[...], incoming, mask4, NT)
    centred = read - left_split(read, mask4) * (1.0 / CHUNK)
    spread = left_split(centred * centred, mask4) * (1.0 / CHUNK)
    gate = 1.0 / (1.0 + jnp.exp(-gate_ref[...].astype(F32)))
    mixed = centred * lax.rsqrt(spread + EPS_GROUP) * gain_ref[...] * gate
    tp = y * nx + x
    blocks[tp] = mixed.astype(BF16)
    total[...] = res_ref[...].astype(F32)
    half = blocks.shape[1] // 2

    def project(slot, part_no, *place):
        rows = pl.ds(part_no * half, half)
        total[rows, :] += jnp.dot(blocks[slot, rows, :], w_ref[slot], preferred_element_type=F32)

    with jax.named_scope("share"):
        sent = share_blocks(blocks, ag_send, ag_recv, y, x, ny, nx, project)
    midway = total[...].astype(BF16)
    mid_ref[...] = midway
    mid_f = midway.astype(F32)
    s_hi, s_lo = halves(mid_f * mid_f)
    ones = jnp.ones((8, wide), BF16)
    sums = dot_dims(ones, s_hi, NT) + dot_dims(ones, s_lo, NT)
    sq_out[...] = sums
    pieces = []
    for i, (a, b) in enumerate(plane):
        copy = remote(sq_out, sq_in.at[i], sq_send.at[i], sq_recv.at[i],
                      y=lax.rem(y + a, ny), x=lax.rem(x + b, nx))
        copy.start()
        pieces.append(copy)
    norm_ref[...] = (mid_f * ngain_ref[...]).astype(BF16)

    def inverse_rms():
        total_sq = sq_out[...]
        for i, copy in enumerate(pieces):
            copy.wait_recv()
            total_sq = total_sq + sq_in[i]
        return lax.rsqrt(total_sq * (1.0 / (wide * ny * nx)) + EPS_NORM)

    return inverse_rms, sent + pieces


def trade_weights(ny, nx, wg_ref, wu_ref, w_a, w_b, wt_s, wt_r):
    y, x = lax.axis_index("y"), lax.axis_index("x")
    ff = wg_ref.shape[1]
    copies = []
    for part, (name, at, n, dst) in enumerate((("x", x, nx, w_a), ("y", y, ny, w_b))):
        cut = ff // n
        for k in ring_order(n):
            to = lax.rem(at + k, n)
            cols = pl.ds(pl.multiple_of(to * cut, cut), cut)
            for which, src in enumerate((wg_ref, wu_ref)):
                copy = remote(src.at[:, cols], dst.at[at, which], wt_s.at[part, which, to],
                              wt_r.at[part, which, at], **{name: to})
                copy.start()
                copies.append(copy)
    for part, (at, n, dst) in enumerate(((x, nx, w_a), (y, ny, w_b))):
        cut = ff // n
        cols = pl.ds(pl.multiple_of(at * cut, cut), cut)
        dst[at, 0] = wg_ref[:, cols]
        dst[at, 1] = wu_ref[:, cols]

    def finish():
        for copy in copies:
            copy.wait_send()
        for part, (at, n, dst) in enumerate(((x, nx, w_a), (y, ny, w_b))):
            for k in ring_order(n):
                src = lax.rem(at + k, n)
                for which in (0, 1):
                    got = dst.at[src, which]
                    remote(got, got, wt_s.at[part, which, 0], wt_r.at[part, which, src], c=1 - lax.axis_index("c")).wait_recv()

    return finish


def prepare_routes(cap, slots, ids_ref, rw_ref, taken, turned, pick_hi, pick_lo):
    tokens = ids_ref.shape[0]
    ids = ids_ref[...]
    id0, id1 = ids[:, 0:1], ids[:, 1:2]
    lane = iota2((tokens, 128), 1)
    hit = jnp.where((lane == id0) | (lane == id1), 1.0, 0.0).astype(BF16)
    tri = jnp.where(iota2((tokens, tokens), 1) < iota2((tokens, tokens), 0), 1.0, 0.0).astype(BF16)
    earlier = dot_dims(tri, hit, NN)

    def slot_of(one):
        rank = jnp.sum(jnp.where(lane == one, earlier, 0.0), axis=1, keepdims=True)
        return one * cap + rank.astype(jnp.int32)

    slot0, slot1 = slot_of(id0), slot_of(id1)
    spot = iota2((tokens, slots), 1)
    hot0, hot1 = spot == slot0, spot == slot1
    take = jnp.where(hot0 | hot1, 1.0, 0.0).astype(BF16)
    rw = rw_ref[...]
    weight = jnp.where(hot0, rw[:, 0:1], 0.0) + jnp.where(hot1, rw[:, 1:2], 0.0)
    w_hi, w_lo = halves(weight)
    pick_hi[...] = w_hi
    pick_lo[...] = w_lo
    taken[...] = take
    eye = (iota2((tokens, tokens), 0) == iota2((tokens, tokens), 1)).astype(F32).astype(BF16)
    turned[...] = dot_dims(take, eye, TN).astype(BF16)


def experts_body(nz, ny, nx, inverse_rms, norm_ref, mid_ref, w_a, w_b, wd_ref, out_ref,
                 taken, turned, pick_hi, pick_lo, going, came, rows_a, rows_b, half_a, half_b, got_a, got_b, own_a, own_b,
                 hid, res, back, scale_out, scale_in, scale_col,
                 go_s, go_r, x_s, x_r, y_s, y_r, a_s, a_r, b_s, b_r, ag_send, ag_recv, re_s, re_r, sc_s, sc_r):
    z, c, y, x = (lax.axis_index(name) for name in ("z", "c", "y", "x"))
    me = 2 * z + c
    tp = y * nx + x
    count, cap, wide = going.shape
    slots = count * cap
    xs, ys = ring_order(nx), ring_order(ny)

    going[...] = dot_dims(turned[...], norm_ref[...], NN).astype(BF16).reshape(going.shape)

    nh = nz // 2
    offs = [0] + [o for d in range(1, nh) for o in (d, nz - d)] + [nh]
    sent = []

    def dispatch(zt, ct):
        copy = remote(going.at[2 * zt + ct], came.at[me], go_s.at[len(sent)], go_r.at[me], z=zt, c=ct)
        copy.start()
        sent.append(copy)

    def dispatch_to(ct):
        for o in offs[1:]:
            dispatch(lax.rem(z + nz - o, nz), ct)

    came[me] = going[me]
    dispatch(z, 1 - c)
    dispatch_to(0)
    group = 128 // cap
    line = jnp.where(c == 0, lax.div(z, nx), lax.rem(z, nx))
    speaks = line == jnp.where(c == 0, y, x)
    place = jnp.where(c == 0, lax.rem(z, nx), lax.div(z, nx))

    def scale_to(e):
        return remote(scale_out.at[lax.div(e, group)], scale_in.at[c, place], sc_s.at[e], sc_r.at[c, place],
                      z=lax.div(e, 2), c=lax.rem(e, 2))

    def tell_scale():
        inv = inverse_rms()
        i_hi, i_rest = halves(inv)
        i_mid, i_lo = halves(inv - i_hi.astype(F32))
        spread = (dot_dims(i_hi, taken[...], NN) + dot_dims(i_mid, taken[...], NN)
                  + dot_dims(i_lo, taken[...], NN))
        for g in range(slots // 128):
            scale_out[g] = spread[:, g * 128 : (g + 1) * 128]

        @pl.when(speaks)
        def _():
            def tell(e, carry):
                @pl.when(e != me)
                def _():
                    scale_to(e).start()

                return carry

            lax.fori_loop(0, count, tell, 0)
            scale_in[c, place] = scale_out[lax.div(me, group)]

    tell_scale()
    dispatch_to(1)

    def take_in(src):
        @pl.when(src != me)
        def _():
            remote(came.at[src], came.at[src], go_s.at[0], go_r.at[src], c=1 - c).wait_recv()

    def onward(t):
        copies = [remote(came.at[2 * t], rows_a.at[x, t], x_s.at[k - 1, t], x_r.at[x, t], x=lax.rem(x + k, nx))
                  for k in xs]
        copies += [remote(came.at[2 * t + 1], rows_b.at[y, t], y_s.at[k - 1, t], y_r.at[y, t], y=lax.rem(y + k, ny))
                   for k in ys]
        return copies

    def receive(t):
        take_in(2 * t)
        take_in(2 * t + 1)
        for copy in onward(t):
            copy.start()

    def settle_a(t):
        ty, tx = lax.div(t, nx), lax.rem(t, nx)
        return remote(half_a.at[t], got_a.at[y, tx], a_s.at[t], a_r.at[y, tx], y=ty)

    def settle_b(t):
        ty, tx = lax.div(t, nx), lax.rem(t, nx)
        return remote(half_b.at[t], got_b.at[x, ty], b_s.at[t], b_r.at[x, ty], x=tx)

    def partials(t):
        ty, tx = lax.div(t, nx), lax.rem(t, nx)
        for part, (places, at, n, rows, recv, w, out, own, mine, spot_own, settle) in enumerate((
            (xs, x, nx, rows_a, x_r, w_a, half_a, own_a, ty == y, tx, settle_a),
            (ys, y, ny, rows_b, y_r, w_b, half_b, own_b, tx == x, ty, settle_b),
        )):
            first = came[2 * t + part]
            gate = jnp.dot(first, w[at, 0], preferred_element_type=F32)
            up = jnp.dot(first, w[at, 1], preferred_element_type=F32)
            for k in places:
                src = lax.rem(at + n - k, n)
                got = rows.at[src, t]
                remote(got, got, go_s.at[0], recv.at[src, t], c=1 - c).wait_recv()
                value = rows[src, t]
                gate = gate + jnp.dot(value, w[src, 0], preferred_element_type=F32)
                up = up + jnp.dot(value, w[src, 1], preferred_element_type=F32)
            cut = gate.shape[1]

            @pl.when(mine)
            def _(own=own, spot_own=spot_own, gate=gate, up=up, cut=cut):
                own[spot_own, :, :cut] = gate
                own[spot_own, :, cut:] = up

            @pl.when(jnp.logical_not(mine))
            def _(out=out, settle=settle, gate=gate, up=up, cut=cut):
                out[t, :, :cut] = gate.astype(BF16)
                out[t, :, cut:] = up.astype(BF16)
                settle(t).start()

    def block_at(i):
        d = lax.div(i + 1, 2)
        off = jnp.where(lax.rem(i, 2) == 1, d, lax.rem(nz - d, nz))
        return lax.rem(z + off, nz)

    def step(j, carry):
        @pl.when(j < nz)
        def _():
            receive(block_at(j))

        @pl.when(j >= LAG)
        def _():
            partials(block_at(j - LAG))

        return carry

    with jax.named_scope("pipeline"):
        lax.fori_loop(0, nz + LAG, step, 0)

    eighth = jnp.full((8, 128), 0.125, BF16)
    with jax.named_scope("scales"):
        for part, m in ((0, nx), (1, ny)):
            for i in range(m):
                from_z = y * nx + i if part == 0 else i * nx + x

                @pl.when(jnp.logical_not(jnp.logical_and(from_z == z, c == part)))
                def _(part=part, i=i):
                    ref = scale_in.at[part, i]
                    remote(ref, ref, sc_s.at[0], sc_r.at[part, i], c=1 - c).wait_recv()

        for part, m in ((0, nx), (1, ny)):
            for i in range(m):
                s_hi, s_rest = halves(scale_in[part, i])
                s_mid, s_lo = halves(scale_in[part, i] - s_hi.astype(F32))
                scale_col[part, i] = dot_dims(s_hi, eighth, TN) + dot_dims(s_mid, eighth, TN) + dot_dims(s_lo, eighth, TN)
    with jax.named_scope("activate"):
        for part, (places, at, n, m, got, recv, own) in enumerate((
            (ys, y, ny, nx, got_a, a_r, own_a),
            (xs, x, nx, ny, got_b, b_r, own_b),
        )):
            for i in range(m):
                factor = scale_col[part, i, pl.ds(pl.multiple_of(lax.rem(me, group) * cap, cap), cap), :]
                total = own[i]
                cut = total.shape[1] // 2
                for k in places:
                    src = lax.rem(at + n - k, n)
                    ref = got.at[src, i]
                    remote(ref, ref, go_s.at[0], recv.at[src, i], c=1 - c).wait_recv()
                    total = total + got[src, i].astype(F32)
                total = total * jnp.concatenate([factor] * (2 * cut // 128), axis=1)
                gate, up = total[:, :cut], total[:, cut:]
                first_row = part * m * cap + i * cap
                hid[tp, first_row : first_row + cap, :] = (gate / (1.0 + jnp.exp(-gate)) * up).astype(BF16)

    def give_back(t, part):
        return remote(res.at[t, part], back.at[me], re_s.at[t, part], re_r.at[me], z=t, c=part)

    seen = {}
    half_rows = hid.shape[1] // 2

    def down(slot, part, dy, dx):
        key = (part, dy if part == 0 else dx)
        seen[key] = seen.get(key, 0) + 1
        n = nx if part == 0 else ny
        if seen[key] < n:
            return
        ry, rx = lax.rem(y + ny - dy, ny), lax.rem(x + nx - dx, nx)
        value = None
        for k in range(n):
            src = ry * nx + k if part == 0 else k * nx + rx
            term = jnp.dot(hid[src, part * half_rows : (part + 1) * half_rows, :], wd_ref[k], preferred_element_type=F32)
            value = term if value is None else value + term
        value = value.astype(BF16)
        for i in range(n):
            t = ry * nx + i if part == 0 else i * nx + rx
            piece = value[i * cap : (i + 1) * cap]
            res[t, part] = piece
            here = jnp.logical_and(t == z, c == part)

            @pl.when(here)
            def _(piece=piece):
                back[me] = piece

            @pl.when(jnp.logical_not(here))
            def _(t=t):
                give_back(t, part).start()

    with jax.named_scope("down"):
        shared = share_blocks(hid, ag_send, ag_recv, y, x, ny, nx, down)

    def collect(src, carry):
        @pl.when(src != me)
        def _():
            remote(back.at[src], back.at[src], re_s.at[0, 0], re_r.at[src], c=1 - c).wait_recv()

        return carry

    with jax.named_scope("collect"):
        lax.fori_loop(0, count, collect, 0)
    rows = back[...].reshape(slots, wide)
    routed = dot_dims(pick_hi[...], rows, NN) + dot_dims(pick_lo[...], rows, NN)
    out_ref[...] = (mid_ref[...].astype(F32) + routed).astype(BF16)

    for copy in sent + shared:
        copy.wait_send()

    def drain(t, carry):
        for copy in onward(t):
            copy.wait_send()

        @pl.when(lax.div(t, nx) != y)
        def _():
            settle_a(t).wait_send()

        @pl.when(lax.rem(t, nx) != x)
        def _():
            settle_b(t).wait_send()

        for part in (0, 1):
            @pl.when(jnp.logical_not(jnp.logical_and(t == z, c == part)))
            def _(part=part):
                give_back(t, part).wait_send()

            e = 2 * t + part

            @pl.when(jnp.logical_and(speaks, e != me))
            def _(e=e):
                scale_to(e).wait_send()

        return carry

    with jax.named_scope("drain"):
        lax.fori_loop(0, nz, drain, 0)


LAG = 6


def layer_body(nz, ny, nx, r_hbm, k_hbm, v_hbm, d_hbm, b_hbm, gate_hbm, gain_ref, res_hbm, w_hbm, ngain_ref,
               ids_ref, rw_ref, wg_hbm, wu_hbm, wd_hbm, out_ref,
               r_ref, k_ref, v_ref, d_ref, b_ref, gate_ref, res_ref, w_ref, wg_ref, wu_ref, wd_ref,
               rd_ref, th_ref, ma_ref, mid_ref, norm_ref, load_s, *rest):
    z, c, y, x = (lax.axis_index(name) for name in ("z", "c", "y", "x"))
    loads = [
        pltpu.make_async_copy(src, dst, load_s.at[i])
        for i, (src, dst) in enumerate((
            (d_hbm, d_ref), (k_hbm, k_ref), (b_hbm, b_ref), (r_hbm, r_ref), (v_hbm, v_ref),
            (gate_hbm, gate_ref), (res_hbm, res_ref), (w_hbm, w_ref),
            (wg_hbm, wg_ref), (wu_hbm, wu_ref), (wd_hbm, wd_ref),
        ))
    ]
    for copy in loads:
        copy.start()
    barrier = pltpu.get_barrier_semaphore()
    plane = [(a, b) for a in range(ny) for b in range(nx) if (a, b) != (0, 0)]
    who = [dict(c=1 - c)]
    who += [dict(z=lax.rem(z + o, nz), c=1 - c if f else c) for o in ring_order(nz) for f in (0, 1)]
    who += [dict(y=lax.rem(y + a, ny), x=lax.rem(x + b, nx)) for a, b in plane]
    for where in who:
        pl.semaphore_signal(barrier, inc=1, device_id=where, device_id_type=MESH)
    for copy in loads[:5]:
        copy.wait()
    with jax.named_scope("mix"):
        mix_body(r_ref, k_ref, v_ref, d_ref, b_ref, rd_ref, th_ref, ma_ref)
    with jax.named_scope("meet"):
        pl.semaphore_wait(barrier, len(who))
        for copy in loads[5:]:
            copy.wait()
    routes = rest[FLOW_SCRATCH + 4 : FLOW_SCRATCH + 8]
    slots, cap = routes[1].shape[0], routes[1].shape[0] // (2 * nz)
    meanwhile = functools.partial(prepare_routes, cap, slots, ids_ref, rw_ref, *routes)
    finish_trade = trade_weights(ny, nx, wg_ref, wu_ref, *rest[FLOW_SCRATCH : FLOW_SCRATCH + 4])
    inverse_rms, sent = flow_body(nz, ny, nx, rd_ref, th_ref, ma_ref, gate_ref, gain_ref, res_ref, ngain_ref, w_ref,
              mid_ref, norm_ref, meanwhile, *rest[:FLOW_SCRATCH])
    finish_trade()
    w_a, w_b = rest[FLOW_SCRATCH], rest[FLOW_SCRATCH + 1]
    experts_body(nz, ny, nx, inverse_rms, norm_ref, mid_ref, w_a, w_b, wd_ref, out_ref,
                 *rest[FLOW_SCRATCH + 4 :])
    for copy in sent:
        copy.wait_send()


FLOW_SCRATCH = 21


def layer(sizes, r, k, v, d, b, gate, gain, res, w, ngain, ids, weights, wg, wu, wd):
    nz, ny, nx = sizes
    tokens, wide = r.shape
    part = wide // 2
    tp = ny * nx
    nstep = max(nz.bit_length() - 2, 0)
    ff = wg.shape[1]
    count = 2 * nz
    cap = 2 * tokens * ids.shape[1] // count
    rows = 2 * cap
    wd = wd.reshape(nx, ff // nx, wide)
    dma = pltpu.SemaphoreType.DMA
    vm = pl.BlockSpec(memory_space=pltpu.VMEM)
    hbm = pl.BlockSpec(memory_space=pl.ANY)
    square = (tokens, wide)
    flow_scratch = [
        pltpu.VMEM((2 * CHUNK, part), BF16),
        pltpu.VMEM((2 * CHUNK, part), BF16),
        pltpu.VMEM((nstep + 1, 2 * CHUNK, part), BF16),
        pltpu.VMEM((max(nstep, 1), 2 * CHUNK, part), BF16),
        pltpu.VMEM((2 * CHUNK, part), BF16),
        pltpu.VMEM((CHUNK, part), BF16),
        pltpu.VMEM((CHUNK, part), BF16),
        pltpu.VMEM((CHUNK, part), BF16),
        pltpu.VMEM((CHUNK, part), BF16),
        pltpu.VMEM((tp,) + square, BF16),
        pltpu.VMEM(square, F32),
        pltpu.VMEM((8, tokens), F32),
        pltpu.VMEM((tp - 1, 8, tokens), F32),
        dma((2,)),
        dma((2, max(nstep, 1))),
        dma((4,)),
        dma((2,)),
        dma((2 * (tp - 1),)),
        dma((2, tp)),
        dma((tp - 1,)),
        dma((tp - 1,)),
    ]
    cut = ff // nx
    trade_scratch = [
        pltpu.VMEM((nx, 2, wide, cut), BF16),
        pltpu.VMEM((ny, 2, wide, cut), BF16),
        dma((2, 2, nx)),
        dma((2, 2, nx)),
    ]
    expert_scratch = [
        pltpu.VMEM((tokens, count * cap), BF16),
        pltpu.VMEM((count * cap, tokens), BF16),
        pltpu.VMEM((tokens, count * cap), BF16),
        pltpu.VMEM((tokens, count * cap), BF16),
        pltpu.VMEM((count, cap, wide), BF16),
        pltpu.VMEM((count, cap, wide), BF16),
        pltpu.VMEM((nx, nz, cap, wide), BF16),
        pltpu.VMEM((ny, nz, cap, wide), BF16),
        pltpu.VMEM((nz, cap, 2 * cut), BF16),
        pltpu.VMEM((nz, cap, 2 * cut), BF16),
        pltpu.VMEM((ny, nx, cap, 2 * cut), BF16),
        pltpu.VMEM((nx, ny, cap, 2 * cut), BF16),
        pltpu.VMEM((nx, cap, 2 * cut), F32),
        pltpu.VMEM((ny, cap, 2 * cut), F32),
        pltpu.VMEM((tp, 2 * nx * cap, cut), BF16),
        pltpu.VMEM((nz, 2, cap, wide), BF16),
        pltpu.VMEM((count, cap, wide), BF16),
        pltpu.VMEM((count * cap // 128, 8, 128), F32),
        pltpu.VMEM((2, nx, 8, 128), F32),
        pltpu.VMEM((2, nx, 128, 128), F32),
        dma((count - 1,)),
        dma((count,)),
        dma((nx - 1, nz)),
        dma((nx, nz)),
        dma((ny - 1, nz)),
        dma((ny, nz)),
        dma((nz,)),
        dma((ny, nx)),
        dma((nz,)),
        dma((nx, ny)),
        dma((2 * (tp - 1),)),
        dma((2, tp)),
        dma((nz, 2)),
        dma((count,)),
        dma((count,)),
        dma((2, nx)),
    ]
    return pl.pallas_call(
        functools.partial(layer_body, nz, ny, nx),
        out_shape=jax.ShapeDtypeStruct(square, BF16),
        in_specs=[hbm] * 6 + [vm] + [hbm] * 2 + [vm] * 3 + [hbm] * 3,
        out_specs=vm,
        scratch_shapes=[pltpu.VMEM(square, BF16)] * 7
        + [
            pltpu.VMEM(w.shape, BF16),
            pltpu.VMEM(wg.shape, BF16),
            pltpu.VMEM(wu.shape, BF16),
            pltpu.VMEM(wd.shape, BF16),
            pltpu.VMEM(square, F32),
            pltpu.VMEM(square, F32),
            pltpu.VMEM((2 * CHUNK, wide), F32),
            pltpu.VMEM(square, BF16),
            pltpu.VMEM(square, BF16),
            dma((11,)),
        ]
        + flow_scratch
        + trade_scratch
        + expert_scratch,
        compiler_params=pltpu.CompilerParams(
            collective_id=0, has_side_effects=True, vmem_limit_bytes=60 * 1024 * 1024
        ),
        name="layer",
    )(r, k, v, d, b, gate, gain, res, w, ngain, ids, weights, wg, wu, wd)


def local(
    receptance,
    key_vectors,
    value_vectors,
    decay_logits,
    rate_logits,
    gate_logits,
    group_gain,
    residual,
    mixer_out,
    norm_gain,
    expert_ids,
    route_weight,
    expert_gate,
    expert_up,
    expert_down,
):
    sizes = tuple(lax.axis_size(name) for name in ("z", "y", "x"))
    features = residual.shape[1]
    return layer(
        sizes,
        receptance,
        key_vectors,
        value_vectors,
        decay_logits,
        rate_logits,
        gate_logits,
        group_gain[None],
        residual,
        mixer_out.reshape(sizes[1] * sizes[2], -1, features),
        norm_gain[None],
        expert_ids,
        route_weight,
        expert_gate[0],
        expert_up[0],
        expert_down[0],
    )


def solution(mesh):
    torus = Mesh(mesh.devices.reshape(16, 2, 4, 4), ("z", "c", "y", "x"))
    return jax.shard_map(
        local,
        mesh=torus,
        in_specs=(
            P(SP, TP),
            P(SP, TP),
            P(SP, TP),
            P(SP, TP),
            P(SP, TP),
            P(SP, TP),
            P(TP),
            P(SP, TP),
            P(None, TP),
            P(TP),
            P(SP, None),
            P(SP, None),
            P(SP, TP, None),
            P(SP, TP, None),
            P(SP, None, TP),
        ),
        out_specs=P(SP, TP),
        check_vma=False,
    )
```
